32 devices in a mesh: ep: 16 (over z, y, x), tp: 2 (over core).
Axes of the slice: x: 2, y: 2, z: 4, core: 2. Of those that a mesh axis runs over, the one named last changes fastest.
Arguments:
- tokens: bfloat16 [256, 2048], P('ep'), may hold values from -6 to 6
- recurrent_state: float32 [256, 4, 128, 256], P('ep', 'tp'), may hold values from -6 to 6
- query_weight: bfloat16 [2048, 512], P(None, 'tp'), may hold values from -0.125 to 0.125
- key_weight: bfloat16 [2048, 512], P(None, 'tp'), may hold values from -0.125 to 0.125
- decay_weight: bfloat16 [2048, 512], P(None, 'tp'), may hold values from -0.5 to 0.5
- value_weight: bfloat16 [2048, 1024], P(None, 'tp'), may hold values from -0.125 to 0.125
- gate_weight: bfloat16 [2048, 1024], P(None, 'tp'), may hold values from -0.125 to 0.125
- head_gain: float32 [256], replicated, may hold values from 0.1 to 1.9
- output_weight: bfloat16 [1024, 2048], P('tp'), may hold values from -0.375 to 0.375
- norm_gain: float32 [2, 2048], replicated, may hold values from 0.1 to 1.9
- norm_bias: float32 [2, 2048], replicated, may hold values from -1.8 to 1.8
- group_router: bfloat16 [2048, 4], replicated, may hold values from -0.125 to 0.125
- router_weight: bfloat16 [2048, 32], replicated, may hold values from -0.125 to 0.125
- routes: int32 [256, 2], P('ep'), may hold values from 0 to 31, as said below
- expert_gate: bfloat16 [32, 2048, 256], P(('ep', 'tp')), may hold values from -0.125 to 0.125
- expert_up: bfloat16 [32, 2048, 256], P(('ep', 'tp')), may hold values from -0.125 to 0.125
- expert_down: bfloat16 [32, 256, 2048], P(('ep', 'tp')), may hold values from -1.5 to 1.5
Outputs:
- new_tokens: bfloat16 [256, 2048], P('ep', 'tp')
- new_state: float32 [256, 4, 128, 256], P('ep', 'tp')
The draws below stay inside these ranges and needn't reach their ends.
Inputs may be any that keep to these rules, and one draw needn't show every extreme that they name: `routes`: each row names two different experts of one group (group g holds the experts g * 8 to g * 8 + 7). In the rows of one device each group is named by the same number of rows and no expert by more than 2 rows; some expert is named by exactly 2 rows of every device.
All inputs are finite; a program needn't handle non-finite values.
Results may differ from the reference program's by a relative error of at most 0.01.
Values may be sent and summed in bfloat16 or wider, within the bound.
A program may use at most 128 MiB of HBM per device.

```python
import jax
import jax.numpy as jnp
from jax import lax

D = 2048
HEADS = 4
DK = 128
DV = 256
EXPERT_FF = 256
GROUPS = 4
TOPK = 2
SEQ_DEV = 16
KW = 512
VW = 1024
EXPERTS = 32
EPG = 8
BATCH = 256
CAP = 2
N_EP = 16
N_TP = 2


def draw_routes(key, part):
    per_group = EXPERTS // GROUPS
    block_keys = jax.random.split(jax.random.fold_in(key, 11), N_EP)

    def permute(subkey):
        return jax.random.permutation(subkey, SEQ_DEV)
    rank_order = jax.vmap(permute)(block_keys).astype(jnp.int32)
    group_id = rank_order % GROUPS
    within_group = rank_order // GROUPS
    offsets = jax.random.randint(jax.random.fold_in(key, 12), (N_EP, GROUPS), 0, per_group).astype(jnp.int32)
    offsets = offsets.at[0, 0].set(0).at[0, GROUPS - 1].set(per_group - 1)
    extra_gap = jax.random.randint(jax.random.fold_in(key, 14), (N_EP, GROUPS), 0, 2).astype(jnp.int32)
    row_offset = jnp.take_along_axis(offsets, group_id, axis=1)
    row_gap = jnp.take_along_axis(extra_gap, group_id, axis=1)
    first_pick = group_id * per_group + (within_group + row_offset) % per_group
    second_pick = group_id * per_group + (within_group + row_offset + 1 + row_gap) % per_group
    flip_bits = jax.random.randint(jax.random.fold_in(key, 13), (N_EP, SEQ_DEV), 0, 2)
    lead_pick = jnp.where(flip_bits == 1, second_pick, first_pick)
    trail_pick = jnp.where(flip_bits == 1, first_pick, second_pick)
    return jnp.stack([lead_pick, trail_pick], axis=-1).reshape(BATCH, 2).astype(jnp.int32)


def level_of(own_key, extent, shards, smallest, largest):
    gain = 1.0
    for position, shards_of in shards:
        steps = jax.random.uniform(jax.random.fold_in(jax.random.fold_in(own_key, 6), position), (shards_of,), jnp.float32, smallest / len(shards), largest / len(shards))
        gain = gain * jnp.repeat(jnp.exp(steps), extent[position] // shards_of).reshape((-1,) + (1,) * (len(extent) - 1 - position))
    return gain


def centred(own_key, extent, width, bound, cuts=(), kind=jnp.bfloat16):
    array = width * jax.random.normal(own_key, extent, jnp.float32)
    if cuts:
        array = array * level_of(own_key, extent, cuts, -0.22, 0.18)
    return jnp.clip(array, -bound, bound).astype(kind)


def setup_inputs(seed: int = 0) -> dict:
    key_list = jax.random.split(jax.random.key(seed), 18)
    return {
        "tokens": centred(key_list[0], (BATCH, D), 1.0, 6.0, ((0, 16),)),
        "recurrent_state": centred(key_list[1], (BATCH, HEADS, DK, DV), 1.0, 6.0, ((0, 16), (1, 2)), jnp.float32),
        "query_weight": centred(key_list[2], (D, KW), D ** -0.5, 0.125, ((1, 2),)),
        "key_weight": centred(key_list[3], (D, KW), D ** -0.5, 0.125, ((1, 2),)),
        "decay_weight": centred(key_list[4], (D, KW), (D // 16) ** -0.5, 0.5, ((1, 2),)),
        "value_weight": centred(key_list[5], (D, VW), D ** -0.5, 0.125, ((1, 2),)),
        "gate_weight": centred(key_list[6], (D, VW), D ** -0.5, 0.125, ((1, 2),)),
        "head_gain": jnp.clip(1.0 + 0.18 * jax.random.normal(key_list[7], (DV,), jnp.float32), 0.1, 1.9),
        "output_weight": centred(key_list[8], (VW, D), (VW // 4) ** -0.5, 0.375, ((0, 2),)),
        "norm_gain": jnp.clip(1.0 + 0.18 * jax.random.normal(key_list[9], (2, D), jnp.float32), 0.1, 1.9),
        "norm_bias": centred(key_list[10], (2, D), 0.3, 1.8, (), jnp.float32),
        "group_router": centred(key_list[11], (D, GROUPS), D ** -0.5, 0.125),
        "router_weight": centred(key_list[12], (D, EXPERTS), D ** -0.5, 0.125),
        "routes": draw_routes(jax.random.fold_in(key_list[17], 71), 0),
        "expert_gate": centred(key_list[14], (EXPERTS, D, EXPERT_FF), D ** -0.5, 0.125, ((0, 32),)),
        "expert_up": centred(key_list[15], (EXPERTS, D, EXPERT_FF), D ** -0.5, 0.125, ((0, 32),)),
        "expert_down": centred(key_list[16], (EXPERTS, EXPERT_FF, D), (EXPERT_FF // 16) ** -0.5, 1.5, ((0, 32),)),
    }


alpha_res = 2.0 ** 0.5
eps_norm = 1e-05

def layer_normed(inputs, gain_row, bias_row):
    centered = inputs - lax.optimization_barrier(jnp.mean(inputs, axis=-1, keepdims=True))
    spread = lax.optimization_barrier(jnp.mean(centered * centered, axis=-1, keepdims=True))
    return centered * lax.rsqrt(spread + eps_norm) * gain_row + bias_row

def rounded_back(values_in):
    return lax.optimization_barrier(values_in.astype(jnp.bfloat16)).astype(jnp.float32)

def reference(tokens, recurrent_state, query_weight, key_weight, decay_weight, value_weight, gate_weight, head_gain, output_weight, norm_gain, norm_bias, group_router, router_weight, routes, expert_gate, expert_up, expert_down):

    def project(weight):
        return jnp.dot(tokens, weight, preferred_element_type=jnp.float32)
    queries = project(query_weight).reshape(BATCH, HEADS, DK) * DK ** (-0.5)
    key_rows = project(key_weight).reshape(BATCH, HEADS, DK)
    value_rows = project(value_weight).reshape(BATCH, HEADS, DV)
    gate_rows = project(gate_weight)
    log_decay = (jax.nn.log_sigmoid(project(decay_weight)) / 16.0).reshape(BATCH, HEADS, DK)
    new_state = jnp.exp(log_decay)[..., None] * recurrent_state + key_rows[..., None] * value_rows[:, :, None, :]
    readout = lax.optimization_barrier(jnp.sum(queries[..., None] * new_state, axis=2))
    norm_scale = lax.rsqrt(lax.optimization_barrier(jnp.mean(readout * readout, axis=-1, keepdims=True)) + eps_norm)
    gated = ((readout * norm_scale * head_gain).reshape(BATCH, VW) * jax.nn.silu(gate_rows)).astype(jnp.bfloat16)
    group_cols = VW // N_TP
    mixed_sum = jnp.zeros((BATCH, D), jnp.float32)
    for part_index in range(N_TP):
        product_part = jnp.dot(gated[:, part_index * group_cols:(part_index + 1) * group_cols], output_weight[part_index * group_cols:(part_index + 1) * group_cols], preferred_element_type=jnp.float32)
        mixed_sum = mixed_sum + rounded_back(product_part)
    hidden = layer_normed(alpha_res * tokens.astype(jnp.float32) + mixed_sum, norm_gain[0], norm_bias[0]).astype(jnp.bfloat16)
    group_logit = jnp.dot(hidden, group_router, preferred_element_type=jnp.float32)
    expert_logit = jnp.dot(hidden, router_weight, preferred_element_type=jnp.float32)
    chosen_group = routes[:, 0] // EPG
    group_hit = chosen_group[:, None] == jnp.arange(GROUPS, dtype=jnp.int32)[None, :]
    own_logit = lax.optimization_barrier(jnp.sum(jnp.where(group_hit, group_logit, 0.0), axis=1, keepdims=True))
    group_share = 1.0 / lax.optimization_barrier(jnp.sum(jnp.exp(group_logit - own_logit), axis=1))
    expert_hit = routes[:, :, None] == jnp.arange(EXPERTS, dtype=jnp.int32)[None, None, :]
    picked = lax.optimization_barrier(jnp.sum(jnp.where(expert_hit, expert_logit[:, None, :], 0.0), axis=2))
    route_weight = group_share[:, None] * jax.nn.sigmoid(picked - picked[:, ::-1])
    flat_routes = routes.reshape(BATCH * TOPK)
    row_limit = N_EP * CAP

    def serve_expert(expert_index):
        hit_index = jnp.nonzero(flat_routes == expert_index, size=row_limit, fill_value=BATCH * TOPK)[0].astype(jnp.int32)
        rows_in = hidden[jnp.minimum(hit_index, BATCH * TOPK - 1) // TOPK]
        gate_part = jnp.dot(rows_in, expert_gate[expert_index], preferred_element_type=jnp.float32)
        up_part = jnp.dot(rows_in, expert_up[expert_index], preferred_element_type=jnp.float32)
        activation = (jax.nn.silu(gate_part) * up_part).astype(jnp.bfloat16)
        combined = jnp.dot(activation, expert_down[expert_index], preferred_element_type=jnp.float32)
        return (hit_index, combined.astype(jnp.bfloat16))
    all_index, all_out = lax.map(serve_expert, jnp.arange(EXPERTS, dtype=jnp.int32))
    expert_out = jnp.zeros((BATCH * TOPK, D), jnp.bfloat16).at[all_index.reshape(-1)].set(all_out.reshape(-1, D), mode='drop')
    routed_sum = lax.optimization_barrier(jnp.sum(route_weight[..., None] * expert_out.reshape(BATCH, TOPK, D).astype(jnp.float32), axis=1))
    new_tokens = layer_normed(alpha_res * hidden.astype(jnp.float32) + routed_sum, norm_gain[1], norm_bias[1]).astype(jnp.bfloat16)
    return (new_tokens, new_state)
```

```python
import functools

import jax
import jax.numpy as jnp
from jax import lax
from jax.experimental import pallas as pl
from jax.experimental.pallas import tpu as pltpu
from jax.sharding import PartitionSpec as P

MESH = pl.DeviceIdType.MESH
alpha_res = 2.0**0.5
eps_norm = 1e-05
F32 = jnp.float32
BF16 = jnp.bfloat16


def dot32(a, b):
    return jnp.dot(a, b, preferred_element_type=F32)


def layer_kernel(
    n_ep,
    n_tp,
    cap,
    chunk,
    tokens_hbm,
    state_hbm,
    wq_hbm,
    wk_hbm,
    wd_hbm,
    wv_hbm,
    wg_hbm,
    gain_hbm,
    wo_hbm,
    norm_gain_hbm,
    norm_bias_hbm,
    group_w_hbm,
    router_w_hbm,
    routes_hbm,
    eg_hbm,
    eu_hbm,
    ed_hbm,
    out_ref,
    fresh,
    tokens,
    state,
    wq,
    wk,
    wd,
    wv,
    wg,
    head_gain,
    wo,
    norm_gain,
    norm_bias,
    group_w,
    router_w,
    routes,
    eg,
    eu,
    ed,
    readout,
    part_mine,
    part_other,
    outgoing,
    arrived,
    results,
    returned,
    stat_mine,
    stat_other,
    in_sem,
    state_sem,
    pair_sem,
    stat_sem,
    go_send,
    go_recv,
    back_send,
    back_recv,
):
    me = lax.axis_index("ep")
    core = lax.axis_index("tp")
    rows, width = tokens.shape
    heads, key_dim, value_dim = state.shape[1:]
    half = width // n_tp
    per_group = router_w.shape[0] // group_w.shape[0]
    slots = n_ep * cap
    chunks = rows // chunk
    unrolled = n_ep <= 32

    def peer(i):
        if not unrolled or n_ep & (n_ep - 1):
            return lax.rem(me + i, n_ep)
        there = me
        bit = 1
        while bit < n_ep:
            if i & bit:
                there = there + bit * (1 - 2 * lax.rem(lax.div(me, bit), 2))
            bit *= 2
        return there

    order = sorted(range(1, n_ep), key=lambda i: -((i & 1) + (i >> 1 & 1) + (i >> 2)))

    def over_peers(body):
        if unrolled:
            for i in order:
                body(i)
        else:

            def step(i, carry):
                body(i)
                return carry

            lax.fori_loop(1, n_ep, step, 0)

    names = (
        ("routes", routes_hbm, routes),
        ("tokens", tokens_hbm, tokens),
        ("wk", wk_hbm, wk),
        ("wd", wd_hbm, wd),
        ("wq", wq_hbm, wq),
        ("wv", wv_hbm, wv),
        ("wg", wg_hbm, wg),
        ("head_gain", gain_hbm, head_gain),
        ("wo", wo_hbm, wo),
        ("norm_gain", norm_gain_hbm, norm_gain),
        ("norm_bias", norm_bias_hbm, norm_bias),
        ("group_w", group_w_hbm, group_w),
        ("router_w", router_w_hbm, router_w),
        ("eg", eg_hbm, eg),
        ("eu", eu_hbm, eu),
        ("ed", ed_hbm, ed),
    )
    load = {
        name: pltpu.make_async_copy(src, dst, in_sem.at[n])
        for n, (name, src, dst) in enumerate(names)
    }
    ins = [
        pltpu.make_async_copy(
            state_hbm.at[pl.ds(n * chunk, chunk)], state.at[pl.ds(n * chunk, chunk)], state_sem.at[n]
        )
        for n in range(chunks)
    ]
    for name in ("routes", "tokens", "wk", "wd", "wq", "wv"):
        load[name].start()
    for one in ins:
        one.start()
    for name in ("wg", "head_gain", "wo", "norm_gain", "norm_bias", "group_w", "router_w"):
        load[name].start()

    barrier = pltpu.get_barrier_semaphore()

    def greet(i):
        for c in range(n_tp):
            pl.semaphore_signal(barrier, inc=1, device_id=(peer(i), c), device_id_type=MESH)

    over_peers(greet)
    for c in range(1, n_tp):
        pl.semaphore_signal(
            barrier, inc=1, device_id=(me, lax.rem(core + c, n_tp)), device_id_type=MESH
        )

    load["routes"].wait()
    first, second = routes[0:1, :], routes[1:2, :]
    before = (
        lax.broadcasted_iota(jnp.int32, (rows, rows), 0)
        < lax.broadcasted_iota(jnp.int32, (rows, rows), 1)
    ).astype(BF16)

    def slot_of(count, to_expert):
        line = lax.broadcasted_iota(jnp.int32, (count, rows), 0)
        expert = to_expert(lax.div(line, cap))
        place = lax.rem(line, cap).astype(F32)
        hit0, hit1 = first == expert, second == expert
        either = jnp.where(hit0, 1.0, jnp.where(hit1, 1.0, 0.0))
        earlier = dot32(either.astype(BF16), before)
        placed = jnp.where(earlier == place, 1.0, 0.0)
        return jnp.where(hit0, placed, 0.0), jnp.where(hit1, placed, 0.0)

    send0, send1 = slot_of(slots, lambda j: j * n_tp + core)
    pick_send = (send0 + send1).astype(BF16)
    back0, back1 = slot_of(slots * n_tp, lambda j: j)

    load["tokens"].wait()
    x = tokens[...]
    load["wk"].wait()
    keys = dot32(x, wk[...])
    load["wd"].wait()
    pre = dot32(x, wd[...])
    decay = jnp.exp((jnp.minimum(pre, 0.0) - jnp.log1p(jnp.exp(-jnp.abs(pre)))) / 16.0)
    load["wq"].wait()
    queries = dot32(x, wq[...]) * key_dim ** (-0.5)
    load["wv"].wait()
    values = dot32(x, wv[...])
    columns = []
    for h in range(heads):
        part = slice(h * key_dim, (h + 1) * key_dim)
        pad = jnp.zeros((key_dim - 3 * rows, key_dim), F32)
        stacked = jnp.concatenate([keys[:, part], decay[:, part], queries[:, part], pad], axis=0)
        columns.append(stacked.T)
    for n in range(chunks):
        ins[n].wait()
        for b in range(n * chunk, (n + 1) * chunk):
            for h in range(heads):
                col = columns[h]
                v = values[b : b + 1, h * value_dim : (h + 1) * value_dim]
                new = (
                    col[:, rows + b : rows + b + 1] * state[b, h]
                    + col[:, b : b + 1] * v
                )
                fresh[b, h] = new
                readout[b : b + 1, h * value_dim : (h + 1) * value_dim] = jnp.sum(
                    col[:, 2 * rows + b : 2 * rows + b + 1] * new, axis=0, keepdims=True
                )
    for name in ("eg", "eu", "ed"):
        load[name].start()
    load["wg"].wait()
    gate = dot32(x, wg[...])
    load["head_gain"].wait()
    gated = []
    for h in range(heads):
        part = slice(h * value_dim, (h + 1) * value_dim)
        r = readout[:, part]
        scale = lax.rsqrt(jnp.mean(r * r, axis=-1, keepdims=True) + eps_norm)
        gated.append((r * scale * head_gain[...] * jax.nn.silu(gate[:, part])).astype(BF16))
    load["wo"].wait()
    part_mine[...] = dot32(jnp.concatenate(gated, axis=1), wo[...]).astype(BF16)

    pl.semaphore_wait(barrier, n_ep * n_tp - 1)
    swap = pltpu.make_async_remote_copy(
        src_ref=part_mine,
        dst_ref=part_other,
        send_sem=pair_sem.at[0],
        recv_sem=pair_sem.at[1],
        device_id=(me, 1 - core),
        device_id_type=MESH,
    )
    swap.start()
    for name in ("norm_gain", "norm_bias", "group_w", "router_w"):
        load[name].wait()
    base = alpha_res * tokens[...].astype(F32) + part_mine[...].astype(F32)
    swap.wait()
    mixed = base + part_other[...].astype(F32)
    centered = mixed - jnp.mean(mixed, axis=-1, keepdims=True)
    spread = jnp.mean(centered * centered, axis=-1, keepdims=True)
    hidden = (
        centered * lax.rsqrt(spread + eps_norm) * norm_gain[0:1, :] + norm_bias[0:1, :]
    ).astype(BF16)

    outgoing[...] = dot32(pick_send, hidden).reshape(n_ep, cap, width).astype(BF16)

    def dispatch(i):
        there = peer(i)
        return pltpu.make_async_remote_copy(
            src_ref=outgoing.at[there],
            dst_ref=arrived.at[me],
            send_sem=go_send.at[i],
            recv_sem=go_recv.at[i],
            device_id=(there, core),
            device_id_type=MESH,
        )

    over_peers(lambda i: dispatch(i).start())
    arrived[me] = outgoing[me]

    across = (((1,), (1,)), ((), ()))
    group_logit = lax.dot_general(group_w[...], hidden, across, preferred_element_type=F32)
    expert_logit = lax.dot_general(router_w[...], hidden, across, preferred_element_type=F32)
    own_group = lax.div(first, per_group)
    group_hit = own_group == lax.broadcasted_iota(jnp.int32, group_logit.shape, 0)
    own_logit = jnp.sum(jnp.where(group_hit, group_logit, 0.0), axis=0, keepdims=True)
    share = 1.0 / jnp.sum(jnp.exp(group_logit - own_logit), axis=0, keepdims=True)
    expert_iota = lax.broadcasted_iota(jnp.int32, expert_logit.shape, 0)
    logit0 = jnp.sum(jnp.where(first == expert_iota, expert_logit, 0.0), axis=0, keepdims=True)
    logit1 = jnp.sum(jnp.where(second == expert_iota, expert_logit, 0.0), axis=0, keepdims=True)
    weighted = back0 * (share * jax.nn.sigmoid(logit0 - logit1)) + back1 * (
        share * jax.nn.sigmoid(logit1 - logit0)
    )
    upper = weighted.astype(BF16)
    lower = (weighted - upper.astype(F32)).astype(BF16)
    mine = jnp.where(core == 0, hidden[:, :half].astype(F32), hidden[:, half:].astype(F32))
    base = alpha_res * mine
    gain = jnp.where(core == 0, norm_gain[1:2, :half], norm_gain[1:2, half:])
    shift = jnp.where(core == 0, norm_bias[1:2, :half], norm_bias[1:2, half:])
    for name in ("eg", "eu", "ed"):
        load[name].wait()

    over_peers(lambda i: dispatch(i).wait())
    rows_in = arrived[...].astype(F32).reshape(slots, width).astype(BF16)
    gate_part = dot32(rows_in, eg[0])
    up_part = dot32(rows_in, eu[0])
    activation = (jax.nn.silu(gate_part) * up_part).astype(BF16)

    def send_back(i, c, from_core):
        there = peer(i)
        return pltpu.make_async_remote_copy(
            src_ref=results.at[c, there],
            dst_ref=returned.at[me * n_tp + core],
            send_sem=back_send.at[c, i],
            recv_sem=back_recv.at[from_core, i],
            device_id=(there, c),
            device_id_type=MESH,
        )

    for c in range(n_tp):
        result = dot32(activation, ed[0, :, c * half : (c + 1) * half])
        results[c] = result.reshape(n_ep, cap, half).astype(BF16)
        over_peers(lambda i: send_back(i, c, core).start())
    beside = pltpu.make_async_remote_copy(
        src_ref=results.at[1 - core, me],
        dst_ref=returned.at[me * n_tp + core],
        send_sem=back_send.at[0, 0],
        recv_sem=back_recv.at[0, 0],
        device_id=(me, 1 - core),
        device_id_type=MESH,
    )
    beside.start()
    returned[me * n_tp + core] = results[core, me]

    def home(i):
        for c in range(n_tp):
            send_back(i, c, c).wait()

    over_peers(home)
    beside.wait()
    fetched = returned[...].astype(F32).reshape(slots * n_tp, half).astype(BF16)
    down = (((0,), (0,)), ((), ()))
    blended = (
        base
        + lax.dot_general(upper, fetched, down, preferred_element_type=F32)
        + lax.dot_general(lower, fetched, down, preferred_element_type=F32)
    )
    total = jnp.sum(blended, axis=1, keepdims=True)
    squares = jnp.sum(blended * blended, axis=1, keepdims=True)
    lane = lax.broadcasted_iota(jnp.int32, stat_mine.shape, 1)
    stats = jnp.where(lane == 0, total, squares)
    stat_mine[...] = stats
    trade = pltpu.make_async_remote_copy(
        src_ref=stat_mine,
        dst_ref=stat_other,
        send_sem=stat_sem.at[0],
        recv_sem=stat_sem.at[1],
        device_id=(me, 1 - core),
        device_id_type=MESH,
    )
    trade.start()
    trade.wait()
    both = stats + stat_other[...]
    row_mean = both[:, 0:1] / width
    spread = both[:, 1:2] / width - row_mean * row_mean
    out_ref[...] = (
        (blended - row_mean) * lax.rsqrt(spread + eps_norm) * gain + shift
    ).astype(BF16)


def store_kernel(chunk, out_ref, fresh, out_hbm, new_hbm, out_sem, new_sem):
    copies = [pltpu.make_async_copy(out_ref, out_hbm, out_sem)]
    for n in range(fresh.shape[0] // chunk):
        part = pl.ds(n * chunk, chunk)
        copies.append(pltpu.make_async_copy(fresh.at[part], new_hbm.at[part], new_sem.at[n]))
    for one in copies:
        one.start()
    for one in copies:
        one.wait()


def on_device(
    n_ep,
    n_tp,
    tokens,
    recurrent_state,
    query_weight,
    key_weight,
    decay_weight,
    value_weight,
    gate_weight,
    head_gain,
    output_weight,
    norm_gain,
    norm_bias,
    group_router,
    router_weight,
    routes,
    expert_gate,
    expert_up,
    expert_down,
):
    rows, width = tokens.shape
    heads, key_dim, value_dim = recurrent_state.shape[1:]
    in_hbm = pl.BlockSpec(memory_space=pltpu.HBM)
    vmem = pl.BlockSpec(memory_space=pltpu.VMEM)
    chunk = 4
    chunks = rows // chunk
    dma = pltpu.SemaphoreType.DMA

    def like(a):
        return pltpu.VMEM(a.shape, a.dtype)

    def pinned(arrays):
        return tuple(pltpu.with_memory_space_constraint(a, pltpu.HBM) for a in arrays)

    experts = router_weight.shape[1]
    cap = 2 * max(1, rows // experts)
    half = width // n_tp
    operands = (
        tokens,
        recurrent_state,
        query_weight,
        key_weight,
        decay_weight,
        value_weight,
        gate_weight,
        head_gain.reshape(1, value_dim),
        output_weight,
        norm_gain,
        norm_bias,
        group_router.T,
        router_weight.T,
        routes.T,
        expert_gate,
        expert_up,
        expert_down,
    )
    new_tokens, new_state = pl.pallas_call(
        functools.partial(layer_kernel, n_ep, n_tp, cap, chunk),
        out_shape=(
            jax.ShapeDtypeStruct((rows, half), BF16),
            jax.ShapeDtypeStruct(recurrent_state.shape, F32),
        ),
        in_specs=[in_hbm] * len(operands),
        out_specs=(vmem, vmem),
        scratch_shapes=[like(a) for a in operands]
        + [
            pltpu.VMEM((rows, heads * value_dim), F32),
            pltpu.VMEM((rows, width), BF16),
            pltpu.VMEM((rows, width), BF16),
            pltpu.VMEM((n_ep, cap, width), BF16),
            pltpu.VMEM((n_ep, cap, width), BF16),
            pltpu.VMEM((n_tp, n_ep, cap, half), BF16),
            pltpu.VMEM((n_ep * n_tp, cap, half), BF16),
            pltpu.VMEM((rows, 128), F32),
            pltpu.VMEM((rows, 128), F32),
            dma((len(operands) - 1,)),
            dma((chunks,)),
            dma((2,)),
            dma((2,)),
            dma((n_ep,)),
            dma((n_ep,)),
            dma((n_tp, n_ep)),
            dma((n_tp, n_ep)),
        ],
        compiler_params=pltpu.CompilerParams(
            collective_id=0, has_side_effects=True, vmem_limit_bytes=40 * 1024 * 1024
        ),
        name="layer",
    )(*pinned(operands))
    return pl.pallas_call(
        functools.partial(store_kernel, chunk),
        out_shape=(
            jax.ShapeDtypeStruct(new_tokens.shape, BF16),
            jax.ShapeDtypeStruct(new_state.shape, F32),
        ),
        in_specs=[vmem, vmem],
        out_specs=(in_hbm, in_hbm),
        scratch_shapes=[dma, dma((chunks,))],
        compiler_params=pltpu.CompilerParams(vmem_limit_bytes=8 * 1024 * 1024),
        name="store",
    )(new_tokens, new_state)


def solution(mesh):
    in_specs = (
        P("ep", None),
        P("ep", "tp", None, None),
        P(None, "tp"),
        P(None, "tp"),
        P(None, "tp"),
        P(None, "tp"),
        P(None, "tp"),
        P(),
        P("tp", None),
        P(),
        P(),
        P(),
        P(),
        P("ep", None),
        P(("ep", "tp"), None, None),
        P(("ep", "tp"), None, None),
        P(("ep", "tp"), None, None),
    )
    out_specs = (P("ep", "tp"), P("ep", "tp", None, None))
    return jax.shard_map(
        functools.partial(on_device, mesh.shape["ep"], mesh.shape["tp"]),
        mesh=mesh,
        in_specs=in_specs,
        out_specs=out_specs,
        check_vma=False,
    )
```

```python
import functools
import math

import jax
import jax.numpy as jnp
from jax import lax
from jax.experimental import pallas as pl
from jax.experimental.pallas import tpu as pltpu
from jax.sharding import PartitionSpec as P

MESH = pl.DeviceIdType.MESH
alpha_res = 2.0**0.5
eps_norm = 1e-05
F32 = jnp.float32
BF16 = jnp.bfloat16
PIECE = 128 * 1024
AHEAD = 8 * 1024 * 1024


def dot32(a, b):
    return jnp.dot(a, b, preferred_element_type=F32)


def pieces(shape, dtype, size=PIECE):
    lead = 1 if len(shape) > 2 and shape[0] == 1 else 0
    whole = math.prod(shape) * jnp.dtype(dtype).itemsize
    count = max(1, min(whole // size, shape[lead] // (16 if len(shape) - lead == 2 else 1)))
    while shape[lead] % count:
        count -= 1
    step = shape[lead] // count
    return [(0,) * lead + (pl.ds(n * step, step),) for n in range(count)]


def layer_kernel(
    n_ep,
    n_tp,
    cap,
    chunk,
    tokens_hbm,
    state_hbm,
    wq_hbm,
    wk_hbm,
    wd_hbm,
    wv_hbm,
    wg_hbm,
    gain_hbm,
    wo_hbm,
    norm_gain_hbm,
    norm_bias_hbm,
    group_w_hbm,
    router_w_hbm,
    routes_hbm,
    eg_hbm,
    eu_hbm,
    ed_hbm,
    out_ref,
    fresh,
    tokens,
    state,
    wq,
    wk,
    wd,
    wv,
    wg,
    head_gain,
    wo,
    norm_gain,
    norm_bias,
    group_w,
    router_w,
    routes,
    eg,
    eu,
    ed,
    readout,
    part_mine,
    part_other,
    outgoing,
    arrived,
    results,
    returned,
    stat_mine,
    stat_other,
    in_sem,
    state_sem,
    pair_sem,
    stat_sem,
    go_send,
    go_recv,
    back_send,
    back_recv,
):
    me = lax.axis_index("ep")
    core = lax.axis_index("tp")
    rows, width = tokens.shape
    heads, key_dim, value_dim = state.shape[1:]
    half = width // n_tp
    per_group = router_w.shape[0] // group_w.shape[0]
    slots = n_ep * cap
    chunks = rows // chunk
    unrolled = n_ep <= 32

    def peer(i):
        if not unrolled or n_ep & (n_ep - 1):
            return lax.rem(me + i, n_ep)
        there = me
        bit = 1
        while bit < n_ep:
            if i & bit:
                there = there + bit * (1 - 2 * lax.rem(lax.div(me, bit), 2))
            bit *= 2
        return there

    order = sorted(range(1, n_ep), key=lambda i: -((i & 1) + (i >> 1 & 1) + (i >> 2)))

    def over_peers(body):
        if unrolled:
            for i in order:
                body(i)
        else:

            def step(i, carry):
                body(i)
                return carry

            lax.fori_loop(1, n_ep, step, 0)

    names = (
        ("routes", routes_hbm, routes),
        ("tokens", tokens_hbm, tokens),
        ("wk", wk_hbm, wk),
        ("wd", wd_hbm, wd),
        ("wq", wq_hbm, wq),
        ("wv", wv_hbm, wv),
        ("wg", wg_hbm, wg),
        ("head_gain", gain_hbm, head_gain),
        ("wo", wo_hbm, wo),
        ("norm_gain", norm_gain_hbm, norm_gain),
        ("norm_bias", norm_bias_hbm, norm_bias),
        ("group_w", group_w_hbm, group_w),
        ("router_w", router_w_hbm, router_w),
        ("eg", eg_hbm, eg),
        ("eu", eu_hbm, eu),
        ("ed", ed_hbm, ed),
    )
    load = {name: (src, dst, in_sem.at[n]) for n, (name, src, dst) in enumerate(names)}
    for n in range(chunks):
        part = pl.ds(n * chunk, chunk)
        load[n] = (state_hbm.at[part], state.at[part], state_sem.at[n])

    def fetch(name):
        src, dst, sem = load[name]
        for part in pieces(src.shape, src.dtype):
            pltpu.make_async_copy(src.at[part], dst.at[part], sem).start()

    def ready(name):
        pltpu.make_async_copy(*load[name]).wait()
        flying.pop(name)
        fetch_more()

    queue = [*("routes", "tokens", "wd", "wq"), *range(chunks), *("wk", "wv", "head_gain", "wg")]
    queue += ["wo", "norm_gain", "norm_bias", "group_w", "router_w", "eg", "eu", "ed"]
    flying = {}

    def fetch_more():
        while queue and sum(flying.values()) < AHEAD:
            name = queue.pop(0)
            src = load[name][0]
            flying[name] = math.prod(src.shape) * jnp.dtype(src.dtype).itemsize
            fetch(name)

    fetch_more()

    barrier = pltpu.get_barrier_semaphore()

    def greet(i):
        for c in range(n_tp):
            pl.semaphore_signal(barrier, inc=1, device_id=(peer(i), c), device_id_type=MESH)

    over_peers(greet)
    for c in range(1, n_tp):
        pl.semaphore_signal(
            barrier, inc=1, device_id=(me, lax.rem(core + c, n_tp)), device_id_type=MESH
        )

    ready("routes")
    first, second = routes[0:1, :], routes[1:2, :]
    before = (
        lax.broadcasted_iota(jnp.int32, (rows, rows), 0)
        < lax.broadcasted_iota(jnp.int32, (rows, rows), 1)
    ).astype(BF16)

    def slot_of(count, to_expert):
        line = lax.broadcasted_iota(jnp.int32, (count, rows), 0)
        expert = to_expert(lax.div(line, cap))
        place = lax.rem(line, cap).astype(F32)
        hit0, hit1 = first == expert, second == expert
        either = jnp.where(hit0, 1.0, jnp.where(hit1, 1.0, 0.0))
        earlier = dot32(either.astype(BF16), before)
        placed = jnp.where(earlier == place, 1.0, 0.0)
        return jnp.where(hit0, placed, 0.0), jnp.where(hit1, placed, 0.0)

    send0, send1 = slot_of(slots, lambda j: j * n_tp + core)
    pick_send = (send0 + send1).astype(BF16)
    back0, back1 = slot_of(slots * n_tp, lambda j: j)

    ready("tokens")
    x = tokens[...]
    ready("wd")
    pre = dot32(x, wd[...])
    decay = jnp.exp((jnp.minimum(pre, 0.0) - jnp.log1p(jnp.exp(-jnp.abs(pre)))) / 16.0)
    ready("wq")
    queries = dot32(x, wq[...]) * key_dim ** (-0.5)
    decayed = queries * decay

    def as_columns(parts):
        pad = jnp.zeros((key_dim - len(parts) * rows, key_dim), F32)
        return [
            jnp.concatenate([p[:, h * key_dim : (h + 1) * key_dim] for p in parts] + [pad], axis=0).T
            for h in range(heads)
        ]

    reading = as_columns([decayed])
    for n in range(chunks):
        ready(n)
        for b in range(n * chunk, (n + 1) * chunk):
            for h in range(heads):
                readout[b : b + 1, h * value_dim : (h + 1) * value_dim] = jnp.sum(
                    reading[h][:, b : b + 1] * state[b, h], axis=0, keepdims=True
                )
    ready("wk")
    keys = dot32(x, wk[...])
    ready("wv")
    values = dot32(x, wv[...])
    both = queries * keys
    ready("wg")
    gate = dot32(x, wg[...])
    ready("head_gain")
    gated = []
    for h in range(heads):
        part = slice(h * value_dim, (h + 1) * value_dim)
        meet = jnp.sum(both[:, h * key_dim : (h + 1) * key_dim], axis=-1, keepdims=True)
        r = readout[:, part] + meet * values[:, part]
        scale = lax.rsqrt(jnp.mean(r * r, axis=-1, keepdims=True) + eps_norm)
        gated.append((r * scale * head_gain[...] * jax.nn.silu(gate[:, part])).astype(BF16))
    ready("wo")
    part_mine[...] = dot32(jnp.concatenate(gated, axis=1), wo[...]).astype(BF16)

    pl.semaphore_wait(barrier, n_ep * n_tp - 1)
    swap = pltpu.make_async_remote_copy(
        src_ref=part_mine,
        dst_ref=part_other,
        send_sem=pair_sem.at[0],
        recv_sem=pair_sem.at[1],
        device_id=(me, 1 - core),
        device_id_type=MESH,
    )
    swap.start()
    for name in ("norm_gain", "norm_bias", "group_w", "router_w"):
        ready(name)
    base = alpha_res * tokens[...].astype(F32) + part_mine[...].astype(F32)
    swap.wait()
    mixed = base + part_other[...].astype(F32)
    centered = mixed - jnp.mean(mixed, axis=-1, keepdims=True)
    spread = jnp.mean(centered * centered, axis=-1, keepdims=True)
    hidden = (
        centered * lax.rsqrt(spread + eps_norm) * norm_gain[0:1, :] + norm_bias[0:1, :]
    ).astype(BF16)

    outgoing[...] = dot32(pick_send, hidden).reshape(n_ep, cap, width).astype(BF16)

    def dispatch(i):
        there = peer(i)
        return pltpu.make_async_remote_copy(
            src_ref=outgoing.at[there],
            dst_ref=arrived.at[me],
            send_sem=go_send,
            recv_sem=go_recv,
            device_id=(there, core),
            device_id_type=MESH,
        )

    others = pl.ds(0, n_ep - 1)
    all_out = pltpu.make_async_remote_copy(
        src_ref=outgoing.at[others],
        dst_ref=arrived.at[others],
        send_sem=go_send,
        recv_sem=go_recv,
        device_id=(peer(1), core),
        device_id_type=MESH,
    )
    over_peers(lambda i: dispatch(i).start())
    arrived[me] = outgoing[me]

    columns = as_columns([keys, decay])
    for b in range(rows):
        for h in range(heads):
            col = columns[h]
            v = values[b : b + 1, h * value_dim : (h + 1) * value_dim]
            fresh[b, h] = col[:, rows + b : rows + b + 1] * state[b, h] + col[:, b : b + 1] * v

    across = (((1,), (1,)), ((), ()))
    group_logit = lax.dot_general(group_w[...], hidden, across, preferred_element_type=F32)
    expert_logit = lax.dot_general(router_w[...], hidden, across, preferred_element_type=F32)
    own_group = lax.div(first, per_group)
    group_hit = own_group == lax.broadcasted_iota(jnp.int32, group_logit.shape, 0)
    own_logit = jnp.sum(jnp.where(group_hit, group_logit, 0.0), axis=0, keepdims=True)
    share = 1.0 / jnp.sum(jnp.exp(group_logit - own_logit), axis=0, keepdims=True)
    expert_iota = lax.broadcasted_iota(jnp.int32, expert_logit.shape, 0)
    logit0 = jnp.sum(jnp.where(first == expert_iota, expert_logit, 0.0), axis=0, keepdims=True)
    logit1 = jnp.sum(jnp.where(second == expert_iota, expert_logit, 0.0), axis=0, keepdims=True)
    weighted = back0 * (share * jax.nn.sigmoid(logit0 - logit1)) + back1 * (
        share * jax.nn.sigmoid(logit1 - logit0)
    )
    upper = weighted.astype(BF16)
    lower = (weighted - upper.astype(F32)).astype(BF16)
    mine = jnp.where(core == 0, hidden[:, :half].astype(F32), hidden[:, half:].astype(F32))
    base = alpha_res * mine
    gain = jnp.where(core == 0, norm_gain[1:2, :half], norm_gain[1:2, half:])
    shift = jnp.where(core == 0, norm_bias[1:2, :half], norm_bias[1:2, half:])
    for name in ("eg", "eu", "ed"):
        ready(name)

    all_out.wait()
    rows_in = arrived[...].astype(F32).reshape(slots, width).astype(BF16)
    gate_part = dot32(rows_in, eg[0])
    up_part = dot32(rows_in, eu[0])
    activation = (jax.nn.silu(gate_part) * up_part).astype(BF16)

    def send_back(i, c):
        there = peer(i)
        return pltpu.make_async_remote_copy(
            src_ref=results.at[c * n_ep + there],
            dst_ref=returned.at[me * n_tp + core],
            send_sem=back_send,
            recv_sem=back_recv,
            device_id=(there, c),
            device_id_type=MESH,
        )

    for c in range(n_tp):
        result = dot32(activation, ed[0, :, c * half : (c + 1) * half])
        results[c * n_ep : (c + 1) * n_ep] = result.reshape(n_ep, cap, half).astype(BF16)
        over_peers(lambda i: send_back(i, c).start())
    pltpu.make_async_remote_copy(
        src_ref=results.at[(1 - core) * n_ep + me],
        dst_ref=returned.at[me * n_tp + core],
        send_sem=back_send,
        recv_sem=back_recv,
        device_id=(me, 1 - core),
        device_id_type=MESH,
    ).start()
    returned[me * n_tp + core] = results[core * n_ep + me]
    others = pl.ds(0, n_ep * n_tp - 1)
    pltpu.make_async_remote_copy(
        src_ref=results.at[others],
        dst_ref=returned.at[others],
        send_sem=back_send,
        recv_sem=back_recv,
        device_id=(me, 1 - core),
        device_id_type=MESH,
    ).wait()
    fetched = returned[...].astype(F32).reshape(slots * n_tp, half).astype(BF16)
    down = (((0,), (0,)), ((), ()))
    blended = (
        base
        + lax.dot_general(upper, fetched, down, preferred_element_type=F32)
        + lax.dot_general(lower, fetched, down, preferred_element_type=F32)
    )
    total = jnp.sum(blended, axis=1, keepdims=True)
    squares = jnp.sum(blended * blended, axis=1, keepdims=True)
    lane = lax.broadcasted_iota(jnp.int32, stat_mine.shape, 1)
    stats = jnp.where(lane == 0, total, squares)
    stat_mine[...] = stats
    trade = pltpu.make_async_remote_copy(
        src_ref=stat_mine,
        dst_ref=stat_other,
        send_sem=stat_sem.at[0],
        recv_sem=stat_sem.at[1],
        device_id=(me, 1 - core),
        device_id_type=MESH,
    )
    trade.start()
    trade.wait()
    both = stats + stat_other[...]
    row_mean = both[:, 0:1] / width
    spread = both[:, 1:2] / width - row_mean * row_mean
    out_ref[...] = (
        (blended - row_mean) * lax.rsqrt(spread + eps_norm) * gain + shift
    ).astype(BF16)


def store_kernel(out_ref, fresh, out_hbm, new_hbm, out_sem, new_sem):
    for part in pieces(fresh.shape, fresh.dtype):
        pltpu.make_async_copy(fresh.at[part], new_hbm.at[part], new_sem).start()
    last = pltpu.make_async_copy(out_ref, out_hbm, out_sem)
    last.start()
    last.wait()
    pltpu.make_async_copy(fresh, new_hbm, new_sem).wait()


def on_device(
    n_ep,
    n_tp,
    tokens,
    recurrent_state,
    query_weight,
    key_weight,
    decay_weight,
    value_weight,
    gate_weight,
    head_gain,
    output_weight,
    norm_gain,
    norm_bias,
    group_router,
    router_weight,
    routes,
    expert_gate,
    expert_up,
    expert_down,
):
    rows, width = tokens.shape
    heads, key_dim, value_dim = recurrent_state.shape[1:]
    in_hbm = pl.BlockSpec(memory_space=pltpu.HBM)
    vmem = pl.BlockSpec(memory_space=pltpu.VMEM)
    chunk = 4
    chunks = rows // chunk
    dma = pltpu.SemaphoreType.DMA

    def like(a):
        return pltpu.VMEM(a.shape, a.dtype)

    def pinned(arrays):
        return tuple(pltpu.with_memory_space_constraint(a, pltpu.HBM) for a in arrays)

    experts = router_weight.shape[1]
    cap = 2 * max(1, rows // experts)
    half = width // n_tp
    operands = (
        tokens,
        recurrent_state,
        query_weight,
        key_weight,
        decay_weight,
        value_weight,
        gate_weight,
        head_gain.reshape(1, value_dim),
        output_weight,
        norm_gain,
        norm_bias,
        group_router.T,
        router_weight.T,
        routes.T,
        expert_gate,
        expert_up,
        expert_down,
    )
    new_tokens, new_state = pl.pallas_call(
        functools.partial(layer_kernel, n_ep, n_tp, cap, chunk),
        out_shape=(
            jax.ShapeDtypeStruct((rows, half), BF16),
            jax.ShapeDtypeStruct(recurrent_state.shape, F32),
        ),
        in_specs=[in_hbm] * len(operands),
        out_specs=(vmem, vmem),
        scratch_shapes=[like(a) for a in operands]
        + [
            pltpu.VMEM((rows, heads * value_dim), F32),
            pltpu.VMEM((rows, width), BF16),
            pltpu.VMEM((rows, width), BF16),
            pltpu.VMEM((n_ep, cap, width), BF16),
            pltpu.VMEM((n_ep, cap, width), BF16),
            pltpu.VMEM((n_tp * n_ep, cap, half), BF16),
            pltpu.VMEM((n_ep * n_tp, cap, half), BF16),
            pltpu.VMEM((rows, 128), F32),
            pltpu.VMEM((rows, 128), F32),
            dma((len(operands) - 1,)),
            dma((chunks,)),
            dma((2,)),
            dma((2,)),
            dma,
            dma,
            dma,
            dma,
        ],
        compiler_params=pltpu.CompilerParams(
            collective_id=0, has_side_effects=True, vmem_limit_bytes=40 * 1024 * 1024
        ),
        name="layer",
    )(*pinned(operands))
    return pl.pallas_call(
        store_kernel,
        out_shape=(
            jax.ShapeDtypeStruct(new_tokens.shape, BF16),
            jax.ShapeDtypeStruct(new_state.shape, F32),
        ),
        in_specs=[vmem, vmem],
        out_specs=(in_hbm, in_hbm),
        scratch_shapes=[dma, dma],
        compiler_params=pltpu.CompilerParams(vmem_limit_bytes=8 * 1024 * 1024),
        name="store",
    )(new_tokens, new_state)


def solution(mesh):
    in_specs = (
        P("ep", None),
        P("ep", "tp", None, None),
        P(None, "tp"),
        P(None, "tp"),
        P(None, "tp"),
        P(None, "tp"),
        P(None, "tp"),
        P(),
        P("tp", None),
        P(),
        P(),
        P(),
        P(),
        P("ep", None),
        P(("ep", "tp"), None, None),
        P(("ep", "tp"), None, None),
        P(("ep", "tp"), None, None),
    )
    out_specs = (P("ep", "tp"), P("ep", "tp", None, None))
    return jax.shard_map(
        functools.partial(on_device, mesh.shape["ep"], mesh.shape["tp"]),
        mesh=mesh,
        in_specs=in_specs,
        out_specs=out_specs,
        check_vma=False,
    )
```

```python
import functools
import math

import jax
import jax.numpy as jnp
from jax import lax
from jax.experimental import pallas as pl
from jax.experimental.pallas import tpu as pltpu
from jax.sharding import PartitionSpec as P

MESH = pl.DeviceIdType.MESH
alpha_res = 2.0**0.5
eps_norm = 1e-05
F32 = jnp.float32
BF16 = jnp.bfloat16
PIECE = 128 * 1024
AHEAD = 8 * 1024 * 1024


def dot32(a, b):
    return jnp.dot(a, b, preferred_element_type=F32)


def pieces(shape, dtype, size=PIECE):
    lead = 1 if len(shape) > 2 and shape[0] == 1 else 0
    whole = math.prod(shape) * jnp.dtype(dtype).itemsize
    count = max(1, min(whole // size, shape[lead] // (16 if len(shape) - lead == 2 else 1)))
    while shape[lead] % count:
        count -= 1
    step = shape[lead] // count
    return [(0,) * lead + (pl.ds(n * step, step),) for n in range(count)]


def layer_kernel(
    n_ep,
    n_tp,
    cap,
    chunk,
    tokens_hbm,
    state_hbm,
    wq_hbm,
    wk_hbm,
    wd_hbm,
    wv_hbm,
    wg_hbm,
    gain_hbm,
    wo_hbm,
    norm_gain_hbm,
    norm_bias_hbm,
    group_w_hbm,
    router_w_hbm,
    routes_hbm,
    eg_hbm,
    eu_hbm,
    ed_hbm,
    out_ref,
    fresh,
    tokens,
    state,
    wq,
    wk,
    wd,
    wv,
    wg,
    head_gain,
    wo,
    norm_gain,
    norm_bias,
    group_w,
    router_w,
    routes,
    eg,
    eu,
    ed,
    readout,
    part_mine,
    part_other,
    outgoing,
    arrived,
    results,
    returned,
    stat_mine,
    stat_other,
    in_sem,
    state_sem,
    pair_sem,
    stat_sem,
    go_send,
    go_recv,
    back_send,
    back_recv,
):
    me = lax.axis_index("ep")
    core = lax.axis_index("tp")
    rows, width = tokens.shape
    heads, key_dim, value_dim = state.shape[1:]
    half = width // n_tp
    per_group = router_w.shape[0] // group_w.shape[0]
    slots = n_ep * cap
    chunks = rows // chunk

    unrolled = n_ep <= 32 and n_ep & (n_ep - 1) == 0

    def peer(i):
        if not unrolled:
            return lax.rem(me + i, n_ep)
        there = me
        bit = 1
        while bit < n_ep:
            if i & bit:
                there = there + bit * (1 - 2 * lax.rem(lax.div(me, bit), 2))
            bit *= 2
        return there

    order = sorted(range(1, n_ep), key=lambda i: -((i & 1) + (i >> 1 & 1) + (i >> 2)))

    def over_peers(body):
        if unrolled:
            for i in order:
                body(i)
        else:

            def step(i, carry):
                body(i)
                return carry

            lax.fori_loop(1, n_ep, step, 0)

    batches = ((0, 1), (1, n_ep // 2 - 1), (n_ep // 2, n_ep // 2))
    own_batch = lax.div(me + n_ep - 1, n_ep) + lax.div(me, n_ep // 2)

    names = (
        ("routes", routes_hbm, routes),
        ("tokens", tokens_hbm, tokens),
        ("wk", wk_hbm, wk),
        ("wd", wd_hbm, wd),
        ("wq", wq_hbm, wq),
        ("wv", wv_hbm, wv),
        ("wg", wg_hbm, wg),
        ("head_gain", gain_hbm, head_gain),
        ("wo", wo_hbm, wo),
        ("norm_gain", norm_gain_hbm, norm_gain),
        ("norm_bias", norm_bias_hbm, norm_bias),
        ("group_w", group_w_hbm, group_w),
        ("router_w", router_w_hbm, router_w),
        ("eg", eg_hbm, eg),
        ("eu", eu_hbm, eu),
        ("ed", ed_hbm, ed),
    )
    load = {name: (src, dst, in_sem.at[n]) for n, (name, src, dst) in enumerate(names)}
    for n in range(chunks):
        part = pl.ds(n * chunk, chunk)
        load[n] = (state_hbm.at[part], state.at[part], state_sem.at[n])

    def fetch(name):
        src, dst, sem = load[name]
        for part in pieces(src.shape, src.dtype):
            pltpu.make_async_copy(src.at[part], dst.at[part], sem).start()

    def ready(name):
        pltpu.make_async_copy(*load[name]).wait()
        flying.pop(name)
        fetch_more()

    queue = [*("routes", "tokens", "wd", "wq"), *range(chunks), *("wk", "wv", "head_gain", "wg")]
    queue += ["wo", "norm_gain", "norm_bias", "group_w", "router_w", "eg", "eu", "ed"]
    flying = {}

    def fetch_more():
        while queue and sum(flying.values()) < AHEAD:
            name = queue.pop(0)
            src = load[name][0]
            flying[name] = math.prod(src.shape) * jnp.dtype(src.dtype).itemsize
            fetch(name)

    fetch_more()

    barrier = pltpu.get_barrier_semaphore()

    def greet(i):
        for c in range(n_tp):
            pl.semaphore_signal(barrier, inc=1, device_id=(peer(i), c), device_id_type=MESH)

    over_peers(greet)
    for c in range(1, n_tp):
        pl.semaphore_signal(
            barrier, inc=1, device_id=(me, lax.rem(core + c, n_tp)), device_id_type=MESH
        )

    ready("routes")
    first, second = routes[0:1, :], routes[1:2, :]
    before = (
        lax.broadcasted_iota(jnp.int32, (rows, rows), 0)
        < lax.broadcasted_iota(jnp.int32, (rows, rows), 1)
    ).astype(BF16)

    def slot_of(count, to_expert):
        line = lax.broadcasted_iota(jnp.int32, (count, rows), 0)
        expert = to_expert(lax.div(line, cap))
        place = lax.rem(line, cap).astype(F32)
        hit0, hit1 = first == expert, second == expert
        either = jnp.where(hit0, 1.0, jnp.where(hit1, 1.0, 0.0))
        earlier = dot32(either.astype(BF16), before)
        placed = jnp.where(earlier == place, 1.0, 0.0)
        return jnp.where(hit0, placed, 0.0), jnp.where(hit1, placed, 0.0)

    send0, send1 = slot_of(slots, lambda j: j * n_tp + core)
    pick_send = (send0 + send1).astype(BF16)
    back0, back1 = slot_of(slots * n_tp, lambda j: j)

    ready("tokens")
    x = tokens[...]
    ready("wd")
    pre = dot32(x, wd[...])
    decay = jnp.exp((jnp.minimum(pre, 0.0) - jnp.log1p(jnp.exp(-jnp.abs(pre)))) / 16.0)
    ready("wq")
    queries = dot32(x, wq[...]) * key_dim ** (-0.5)
    decayed = queries * decay

    def as_columns(parts):
        pad = jnp.zeros((key_dim - len(parts) * rows, key_dim), F32)
        return [
            jnp.concatenate([p[:, h * key_dim : (h + 1) * key_dim] for p in parts] + [pad], axis=0).T
            for h in range(heads)
        ]

    reading = as_columns([decayed])
    for n in range(chunks):
        ready(n)
        for b in range(n * chunk, (n + 1) * chunk):
            for h in range(heads):
                readout[b : b + 1, h * value_dim : (h + 1) * value_dim] = jnp.sum(
                    reading[h][:, b : b + 1] * state[b, h], axis=0, keepdims=True
                )
    ready("wk")
    keys = dot32(x, wk[...])
    ready("wv")
    values = dot32(x, wv[...])
    both = queries * keys
    ready("wg")
    gate = dot32(x, wg[...])
    ready("head_gain")
    gated = []
    for h in range(heads):
        part = slice(h * value_dim, (h + 1) * value_dim)
        meet = jnp.sum(both[:, h * key_dim : (h + 1) * key_dim], axis=-1, keepdims=True)
        r = readout[:, part] + meet * values[:, part]
        scale = lax.rsqrt(jnp.mean(r * r, axis=-1, keepdims=True) + eps_norm)
        gated.append((r * scale * head_gain[...] * jax.nn.silu(gate[:, part])).astype(BF16))
    ready("wo")
    part_mine[...] = dot32(jnp.concatenate(gated, axis=1), wo[...]).astype(BF16)

    pl.semaphore_wait(barrier, n_ep * n_tp - 1)
    swap = pltpu.make_async_remote_copy(
        src_ref=part_mine,
        dst_ref=part_other,
        send_sem=pair_sem.at[0],
        recv_sem=pair_sem.at[1],
        device_id=(me, 1 - core),
        device_id_type=MESH,
    )
    swap.start()
    for name in ("norm_gain", "norm_bias", "group_w", "router_w"):
        ready(name)
    base = alpha_res * tokens[...].astype(F32) + part_mine[...].astype(F32)
    swap.wait()
    mixed = base + part_other[...].astype(F32)
    centered = mixed - jnp.mean(mixed, axis=-1, keepdims=True)
    spread = jnp.mean(centered * centered, axis=-1, keepdims=True)
    hidden = (
        centered * lax.rsqrt(spread + eps_norm) * norm_gain[0:1, :] + norm_bias[0:1, :]
    ).astype(BF16)

    outgoing[...] = dot32(pick_send, hidden).reshape(n_ep, cap, width).astype(BF16)

    def dispatch(i):
        there = peer(i)
        return pltpu.make_async_remote_copy(
            src_ref=outgoing.at[there],
            dst_ref=arrived.at[me],
            send_sem=go_send,
            recv_sem=go_recv.at[own_batch],
            device_id=(there, core),
            device_id_type=MESH,
        )

    over_peers(lambda i: dispatch(i).start())
    arrived[me] = outgoing[me]

    columns = as_columns([keys, decay])
    for b in range(rows):
        for h in range(heads):
            col = columns[h]
            v = values[b : b + 1, h * value_dim : (h + 1) * value_dim]
            fresh[b, h] = col[:, rows + b : rows + b + 1] * state[b, h] + col[:, b : b + 1] * v

    across = (((1,), (1,)), ((), ()))
    group_logit = lax.dot_general(group_w[...], hidden, across, preferred_element_type=F32)
    expert_logit = lax.dot_general(router_w[...], hidden, across, preferred_element_type=F32)
    own_group = lax.div(first, per_group)
    group_hit = own_group == lax.broadcasted_iota(jnp.int32, group_logit.shape, 0)
    own_logit = jnp.sum(jnp.where(group_hit, group_logit, 0.0), axis=0, keepdims=True)
    share = 1.0 / jnp.sum(jnp.exp(group_logit - own_logit), axis=0, keepdims=True)
    expert_iota = lax.broadcasted_iota(jnp.int32, expert_logit.shape, 0)
    logit0 = jnp.sum(jnp.where(first == expert_iota, expert_logit, 0.0), axis=0, keepdims=True)
    logit1 = jnp.sum(jnp.where(second == expert_iota, expert_logit, 0.0), axis=0, keepdims=True)
    weighted = back0 * (share * jax.nn.sigmoid(logit0 - logit1)) + back1 * (
        share * jax.nn.sigmoid(logit1 - logit0)
    )
    upper = weighted.astype(BF16)
    lower = (weighted - upper.astype(F32)).astype(BF16)
    mine = jnp.where(core == 0, hidden[:, :half].astype(F32), hidden[:, half:].astype(F32))
    base = alpha_res * mine
    gain = jnp.where(core == 0, norm_gain[1:2, :half], norm_gain[1:2, half:])
    shift = jnp.where(core == 0, norm_bias[1:2, :half], norm_bias[1:2, half:])
    for name in ("eg", "eu", "ed"):
        ready(name)

    def send_back(there, c):
        return pltpu.make_async_remote_copy(
            src_ref=results.at[c * n_ep + there],
            dst_ref=returned.at[me * n_tp + core],
            send_sem=back_send,
            recv_sem=back_recv,
            device_id=(there, c),
            device_id_type=MESH,
        )

    def landed(batch, count):
        some = arrived.at[pl.ds(0, count)]
        pltpu.make_async_copy(some, some, go_recv.at[batch]).wait()

    def serve(batch):
        start, size = batches[batch]
        if size > 1:
            pl.when(own_batch == batch)(lambda: landed(batch, size - 1))
        pl.when(own_batch != batch)(lambda: landed(batch, size))
        rows_in = arrived[start : start + size].astype(F32)
        rows_in = rows_in.reshape(size * cap, width).astype(BF16)
        gate_part = dot32(rows_in, eg[0])
        up_part = dot32(rows_in, eu[0])
        activation = (jax.nn.silu(gate_part) * up_part).astype(BF16)
        for c in range(n_tp):
            at = c * n_ep + start
            result = dot32(activation, ed[0, :, c * half : (c + 1) * half])
            results[at : at + size] = result.reshape(size, cap, half).astype(BF16)
            if size == 1:
                pl.when(own_batch != batch)(lambda: send_back(start, c).start())
                continue

            def back(i):
                there = peer(i)
                pl.when((there >= start) & (there < start + size))(lambda: send_back(there, c).start())

            over_peers(back)

    serve(0)
    serve(1)
    serve(2)
    pltpu.make_async_remote_copy(
        src_ref=results.at[(1 - core) * n_ep + me],
        dst_ref=returned.at[me * n_tp + core],
        send_sem=back_send,
        recv_sem=back_recv,
        device_id=(me, 1 - core),
        device_id_type=MESH,
    ).start()
    returned[me * n_tp + core] = results[core * n_ep + me]
    others = pl.ds(0, n_ep - 1)
    pltpu.make_async_copy(outgoing.at[others], outgoing.at[others], go_send).wait()
    others = pl.ds(0, n_ep * n_tp - 1)
    pltpu.make_async_copy(returned.at[others], returned.at[others], back_recv).wait()
    pltpu.make_async_copy(results.at[others], results.at[others], back_send).wait()
    fetched = returned[...].astype(F32).reshape(slots * n_tp, half).astype(BF16)
    down = (((0,), (0,)), ((), ()))
    blended = (
        base
        + lax.dot_general(upper, fetched, down, preferred_element_type=F32)
        + lax.dot_general(lower, fetched, down, preferred_element_type=F32)
    )
    total = jnp.sum(blended, axis=1, keepdims=True)
    squares = jnp.sum(blended * blended, axis=1, keepdims=True)
    lane = lax.broadcasted_iota(jnp.int32, stat_mine.shape, 1)
    stats = jnp.where(lane == 0, total, squares)
    stat_mine[...] = stats
    trade = pltpu.make_async_remote_copy(
        src_ref=stat_mine,
        dst_ref=stat_other,
        send_sem=stat_sem.at[0],
        recv_sem=stat_sem.at[1],
        device_id=(me, 1 - core),
        device_id_type=MESH,
    )
    trade.start()
    trade.wait()
    both = stats + stat_other[...]
    row_mean = both[:, 0:1] / width
    spread = both[:, 1:2] / width - row_mean * row_mean
    out_ref[...] = (
        (blended - row_mean) * lax.rsqrt(spread + eps_norm) * gain + shift
    ).astype(BF16)


def store_kernel(out_ref, fresh, out_hbm, new_hbm, out_sem, new_sem):
    for part in pieces(fresh.shape, fresh.dtype):
        pltpu.make_async_copy(fresh.at[part], new_hbm.at[part], new_sem).start()
    last = pltpu.make_async_copy(out_ref, out_hbm, out_sem)
    last.start()
    last.wait()
    pltpu.make_async_copy(fresh, new_hbm, new_sem).wait()


def on_device(
    n_ep,
    n_tp,
    tokens,
    recurrent_state,
    query_weight,
    key_weight,
    decay_weight,
    value_weight,
    gate_weight,
    head_gain,
    output_weight,
    norm_gain,
    norm_bias,
    group_router,
    router_weight,
    routes,
    expert_gate,
    expert_up,
    expert_down,
):
    rows, width = tokens.shape
    heads, key_dim, value_dim = recurrent_state.shape[1:]
    in_hbm = pl.BlockSpec(memory_space=pltpu.HBM)
    vmem = pl.BlockSpec(memory_space=pltpu.VMEM)
    chunk = 4
    chunks = rows // chunk
    dma = pltpu.SemaphoreType.DMA

    def like(a):
        return pltpu.VMEM(a.shape, a.dtype)

    def pinned(arrays):
        return tuple(pltpu.with_memory_space_constraint(a, pltpu.HBM) for a in arrays)

    experts = router_weight.shape[1]
    cap = 2 * max(1, rows // experts)
    half = width // n_tp
    operands = (
        tokens,
        recurrent_state,
        query_weight,
        key_weight,
        decay_weight,
        value_weight,
        gate_weight,
        head_gain.reshape(1, value_dim),
        output_weight,
        norm_gain,
        norm_bias,
        group_router.T,
        router_weight.T,
        routes.T,
        expert_gate,
        expert_up,
        expert_down,
    )
    new_tokens, new_state = pl.pallas_call(
        functools.partial(layer_kernel, n_ep, n_tp, cap, chunk),
        out_shape=(
            jax.ShapeDtypeStruct((rows, half), BF16),
            jax.ShapeDtypeStruct(recurrent_state.shape, F32),
        ),
        in_specs=[in_hbm] * len(operands),
        out_specs=(vmem, vmem),
        scratch_shapes=[like(a) for a in operands]
        + [
            pltpu.VMEM((rows, heads * value_dim), F32),
            pltpu.VMEM((rows, width), BF16),
            pltpu.VMEM((rows, width), BF16),
            pltpu.VMEM((n_ep, cap, width), BF16),
            pltpu.VMEM((n_ep, cap, width), BF16),
            pltpu.VMEM((n_tp * n_ep, cap, half), BF16),
            pltpu.VMEM((n_ep * n_tp, cap, half), BF16),
            pltpu.VMEM((rows, 128), F32),
            pltpu.VMEM((rows, 128), F32),
            dma((len(operands) - 1,)),
            dma((chunks,)),
            dma((2,)),
            dma((2,)),
            dma,
            dma((3,)),
            dma,
            dma,
        ],
        compiler_params=pltpu.CompilerParams(
            collective_id=0, has_side_effects=True, vmem_limit_bytes=40 * 1024 * 1024
        ),
        name="layer",
    )(*pinned(operands))
    return pl.pallas_call(
        store_kernel,
        out_shape=(
            jax.ShapeDtypeStruct(new_tokens.shape, BF16),
            jax.ShapeDtypeStruct(new_state.shape, F32),
        ),
        in_specs=[vmem, vmem],
        out_specs=(in_hbm, in_hbm),
        scratch_shapes=[dma, dma],
        compiler_params=pltpu.CompilerParams(vmem_limit_bytes=8 * 1024 * 1024),
        name="store",
    )(new_tokens, new_state)


def solution(mesh):
    in_specs = (
        P("ep", None),
        P("ep", "tp", None, None),
        P(None, "tp"),
        P(None, "tp"),
        P(None, "tp"),
        P(None, "tp"),
        P(None, "tp"),
        P(),
        P("tp", None),
        P(),
        P(),
        P(),
        P(),
        P("ep", None),
        P(("ep", "tp"), None, None),
        P(("ep", "tp"), None, None),
        P(("ep", "tp"), None, None),
    )
    out_specs = (P("ep", "tp"), P("ep", "tp", None, None))
    return jax.shard_map(
        functools.partial(on_device, mesh.shape["ep"], mesh.shape["tp"]),
        mesh=mesh,
        in_specs=in_specs,
        out_specs=out_specs,
        check_vma=False,
    )
```

```python
import functools
import math

import jax
import jax.numpy as jnp
from jax import lax
from jax.experimental import pallas as pl
from jax.experimental.pallas import tpu as pltpu
from jax.sharding import PartitionSpec as P

MESH = pl.DeviceIdType.MESH
alpha_res = 2.0**0.5
eps_norm = 1e-05
F32 = jnp.float32
BF16 = jnp.bfloat16
PIECE = 256 * 1024
AHEAD = 7 * 1024 * 1024


def dot32(a, b):
    return jnp.dot(a, b, preferred_element_type=F32)


def pieces(shape, dtype, size=PIECE):
    lead = 1 if len(shape) > 2 and shape[0] == 1 else 0
    whole = math.prod(shape) * jnp.dtype(dtype).itemsize
    count = max(1, min(whole // size, shape[lead] // (16 if len(shape) - lead == 2 else 1)))
    while shape[lead] % count:
        count -= 1
    step = shape[lead] // count
    return [(0,) * lead + (pl.ds(n * step, step),) for n in range(count)]


def layer_kernel(
    n_ep,
    n_tp,
    cap,
    chunk,
    tokens_hbm,
    state_hbm,
    wq_hbm,
    wk_hbm,
    wd_hbm,
    wv_hbm,
    wg_hbm,
    gain_hbm,
    wo_hbm,
    norm_gain_hbm,
    norm_bias_hbm,
    group_w_hbm,
    router_w_hbm,
    routes_hbm,
    eg_hbm,
    eu_hbm,
    ed_hbm,
    out_ref,
    fresh,
    tokens,
    state,
    wq,
    wk,
    wd,
    wv,
    wg,
    head_gain,
    wo,
    norm_gain,
    norm_bias,
    group_w,
    router_w,
    routes,
    eg,
    eu,
    ed,
    readout,
    part_mine,
    part_other,
    outgoing,
    arrived,
    results,
    returned,
    stat_mine,
    stat_other,
    in_sem,
    state_sem,
    pair_sem,
    stat_sem,
    go_send,
    go_recv,
    back_send,
    back_recv,
):
    me = lax.axis_index("ep")
    core = lax.axis_index("tp")
    rows, width = tokens.shape
    heads, key_dim, value_dim = state.shape[1:]
    half = width // n_tp
    per_group = router_w.shape[0] // group_w.shape[0]
    slots = n_ep * cap
    chunks = rows // chunk

    unrolled = n_ep <= 32 and n_ep & (n_ep - 1) == 0

    own_side = lax.div(me, n_ep // 2)

    def peer(i):
        if not unrolled:
            return lax.rem(me + i, n_ep)
        planes = n_ep // 4
        if i >= n_ep // 2 and planes > 1:
            plane = i // 4 + own_side * (planes - 1 - 2 * (i // 4))
            there = plane * 4 + lax.rem(me, 4)
            i = i % 4
        else:
            there = me
        bit = 1
        while bit < n_ep:
            if i & bit:
                there = there + bit * (1 - 2 * lax.rem(lax.div(me, bit), 2))
            bit *= 2
        return there

    order = sorted(range(1, n_ep), key=lambda i: -((i & 1) + (i >> 1 & 1) + (i >> 2)))

    def over_peers(body):
        if unrolled:
            for i in order:
                body(i)
        else:

            def step(i, carry):
                body(i)
                return carry

            lax.fori_loop(1, n_ep, step, 0)

    batches = ((0, 1), (1, n_ep // 4 - 1), (n_ep // 4, n_ep // 4), (n_ep // 2, n_ep // 2))
    own_batch = lax.div(me + n_ep - 1, n_ep) + lax.div(me, n_ep // 4) - lax.div(me, 3 * (n_ep // 4))

    names = (
        ("routes", routes_hbm, routes),
        ("tokens", tokens_hbm, tokens),
        ("wk", wk_hbm, wk),
        ("wd", wd_hbm, wd),
        ("wq", wq_hbm, wq),
        ("wv", wv_hbm, wv),
        ("wg", wg_hbm, wg),
        ("head_gain", gain_hbm, head_gain),
        ("wo", wo_hbm, wo),
        ("norm_gain", norm_gain_hbm, norm_gain),
        ("norm_bias", norm_bias_hbm, norm_bias),
        ("group_w", group_w_hbm, group_w),
        ("router_w", router_w_hbm, router_w),
        ("eg", eg_hbm, eg),
        ("eu", eu_hbm, eu),
        ("ed", ed_hbm, ed),
    )
    load = {name: (src, dst, in_sem.at[n]) for n, (name, src, dst) in enumerate(names)}
    for n in range(chunks):
        part = pl.ds(n * chunk, chunk)
        load[n] = (state_hbm.at[part], state.at[part], state_sem.at[n])

    def fetch(name):
        src, dst, sem = load[name]
        for part in pieces(src.shape, src.dtype):
            pltpu.make_async_copy(src.at[part], dst.at[part], sem).start()

    def ready(name):
        pltpu.make_async_copy(*load[name]).wait()
        flying.pop(name)
        fetch_more()

    queue = [*("routes", "tokens", "wd", "wq"), *range(chunks), *("wk", "wv", "head_gain", "wg")]
    queue += ["wo", "norm_gain", "norm_bias", "group_w", "router_w", "eg", "eu", "ed"]
    flying = {}

    def fetch_more():
        while queue and sum(flying.values()) < AHEAD:
            name = queue.pop(0)
            src = load[name][0]
            flying[name] = math.prod(src.shape) * jnp.dtype(src.dtype).itemsize
            fetch(name)

    fetch_more()

    barrier = pltpu.get_barrier_semaphore()

    def greet(i):
        for c in range(n_tp):
            pl.semaphore_signal(barrier, inc=1, device_id=(peer(i), c), device_id_type=MESH)

    over_peers(greet)
    for c in range(1, n_tp):
        pl.semaphore_signal(
            barrier, inc=1, device_id=(me, lax.rem(core + c, n_tp)), device_id_type=MESH
        )

    ready("routes")
    first, second = routes[0:1, :], routes[1:2, :]
    before = (
        lax.broadcasted_iota(jnp.int32, (rows, rows), 0)
        < lax.broadcasted_iota(jnp.int32, (rows, rows), 1)
    ).astype(BF16)

    def slot_of(count, to_expert):
        line = lax.broadcasted_iota(jnp.int32, (count, rows), 0)
        expert = to_expert(lax.div(line, cap))
        place = lax.rem(line, cap).astype(F32)
        hit0, hit1 = first == expert, second == expert
        either = jnp.where(hit0, 1.0, jnp.where(hit1, 1.0, 0.0))
        earlier = dot32(either.astype(BF16), before)
        placed = jnp.where(earlier == place, 1.0, 0.0)
        return jnp.where(hit0, placed, 0.0), jnp.where(hit1, placed, 0.0)

    send0, send1 = slot_of(slots, lambda j: j * n_tp + core)
    pick_send = (send0 + send1).astype(BF16)
    back0, back1 = slot_of(slots * n_tp, lambda j: j)

    ready("tokens")
    x = tokens[...]
    ready("wd")
    pre = dot32(x, wd[...])
    decay = jnp.exp((jnp.minimum(pre, 0.0) - jnp.log1p(jnp.exp(-jnp.abs(pre)))) / 16.0)
    ready("wq")
    queries = dot32(x, wq[...]) * key_dim ** (-0.5)
    decayed = queries * decay

    def as_columns(parts):
        pad = jnp.zeros((key_dim - len(parts) * rows, key_dim), F32)
        return [
            jnp.concatenate([p[:, h * key_dim : (h + 1) * key_dim] for p in parts] + [pad], axis=0).T
            for h in range(heads)
        ]

    reading = as_columns([decayed])
    for n in range(chunks):
        ready(n)
        for b in range(n * chunk, (n + 1) * chunk):
            for h in range(heads):
                readout[b : b + 1, h * value_dim : (h + 1) * value_dim] = jnp.sum(
                    reading[h][:, b : b + 1] * state[b, h], axis=0, keepdims=True
                )
    ready("wk")
    keys = dot32(x, wk[...])
    ready("wv")
    values = dot32(x, wv[...])
    both = queries * keys
    ready("wg")
    gate = dot32(x, wg[...])
    ready("head_gain")
    gated = []
    for h in range(heads):
        part = slice(h * value_dim, (h + 1) * value_dim)
        meet = jnp.sum(both[:, h * key_dim : (h + 1) * key_dim], axis=-1, keepdims=True)
        r = readout[:, part] + meet * values[:, part]
        scale = lax.rsqrt(jnp.mean(r * r, axis=-1, keepdims=True) + eps_norm)
        gated.append((r * scale * head_gain[...] * jax.nn.silu(gate[:, part])).astype(BF16))
    ready("wo")
    gated = jnp.concatenate(gated, axis=1)
    for c in range(n_tp):
        part = slice(c * half, (c + 1) * half)
        part_mine[:, part] = dot32(gated, wo[:, part]).astype(BF16)

    pl.semaphore_wait(barrier, n_ep * n_tp - 1)
    swap = pltpu.make_async_remote_copy(
        src_ref=part_mine,
        dst_ref=part_other,
        send_sem=pair_sem.at[0],
        recv_sem=pair_sem.at[1],
        device_id=(me, 1 - core),
        device_id_type=MESH,
    )
    swap.start()
    for name in ("norm_gain", "norm_bias", "group_w", "router_w"):
        ready(name)
    base = alpha_res * tokens[...].astype(F32) + part_mine[...].astype(F32)
    swap.wait()
    mixed = base + part_other[...].astype(F32)
    centered = mixed - jnp.mean(mixed, axis=-1, keepdims=True)
    spread = jnp.mean(centered * centered, axis=-1, keepdims=True)
    hidden = (
        centered * lax.rsqrt(spread + eps_norm) * norm_gain[0:1, :] + norm_bias[0:1, :]
    ).astype(BF16)

    outgoing[...] = dot32(pick_send, hidden).reshape(n_ep, cap, width).astype(BF16)

    def dispatch(i):
        there = peer(i)
        return pltpu.make_async_remote_copy(
            src_ref=outgoing.at[there],
            dst_ref=arrived.at[me],
            send_sem=go_send,
            recv_sem=go_recv.at[own_batch],
            device_id=(there, core),
            device_id_type=MESH,
        )

    over_peers(lambda i: dispatch(i).start())
    arrived[me] = outgoing[me]

    @pl.when(me >= 0)
    def _():
        columns = as_columns([keys, decay])
        for b in range(rows):
            for h in range(heads):
                col = columns[h]
                v = values[b : b + 1, h * value_dim : (h + 1) * value_dim]
                fresh[b, h] = col[:, rows + b : rows + b + 1] * state[b, h] + col[:, b : b + 1] * v

    across = (((1,), (1,)), ((), ()))
    group_logit = lax.dot_general(group_w[...], hidden, across, preferred_element_type=F32)
    expert_logit = lax.dot_general(router_w[...], hidden, across, preferred_element_type=F32)
    own_group = lax.div(first, per_group)
    group_hit = own_group == lax.broadcasted_iota(jnp.int32, group_logit.shape, 0)
    own_logit = jnp.sum(jnp.where(group_hit, group_logit, 0.0), axis=0, keepdims=True)
    share = 1.0 / jnp.sum(jnp.exp(group_logit - own_logit), axis=0, keepdims=True)
    expert_iota = lax.broadcasted_iota(jnp.int32, expert_logit.shape, 0)
    logit0 = jnp.sum(jnp.where(first == expert_iota, expert_logit, 0.0), axis=0, keepdims=True)
    logit1 = jnp.sum(jnp.where(second == expert_iota, expert_logit, 0.0), axis=0, keepdims=True)
    weighted = back0 * (share * jax.nn.sigmoid(logit0 - logit1)) + back1 * (
        share * jax.nn.sigmoid(logit1 - logit0)
    )
    upper = weighted.astype(BF16)
    lower = (weighted - upper.astype(F32)).astype(BF16)
    mine = jnp.where(core == 0, hidden[:, :half].astype(F32), hidden[:, half:].astype(F32))
    base = alpha_res * mine
    gain = jnp.where(core == 0, norm_gain[1:2, :half], norm_gain[1:2, half:])
    shift = jnp.where(core == 0, norm_bias[1:2, :half], norm_bias[1:2, half:])
    for name in ("eg", "eu", "ed"):
        ready(name)

    def send_back(there, c):
        return pltpu.make_async_remote_copy(
            src_ref=results.at[c * n_ep + there],
            dst_ref=returned.at[me * n_tp + core],
            send_sem=back_send,
            recv_sem=back_recv,
            device_id=(there, c),
            device_id_type=MESH,
        )

    def landed(batch, count):
        some = arrived.at[pl.ds(0, count)]
        pltpu.make_async_copy(some, some, go_recv.at[batch]).wait()

    def serve(batch):
        start, size = batches[batch]
        if size > 1:
            pl.when(own_batch == batch)(lambda: landed(batch, size - 1))
        pl.when(own_batch != batch)(lambda: landed(batch, size))
        rows_in = arrived[start : start + size].astype(F32)
        rows_in = rows_in.reshape(size * cap, width).astype(BF16)
        gate_part = dot32(rows_in, eg[0])
        up_part = dot32(rows_in, eu[0])
        activation = (jax.nn.silu(gate_part) * up_part).astype(BF16)
        for c in range(n_tp):
            at = c * n_ep + start
            result = dot32(activation, ed[0, :, c * half : (c + 1) * half])
            results[at : at + size] = result.reshape(size, cap, half).astype(BF16)
            if size == 1:
                pl.when(own_batch != batch)(lambda: send_back(start, c).start())
                continue

            def back(i):
                there = peer(i)
                pl.when((there >= start) & (there < start + size))(lambda: send_back(there, c).start())

            over_peers(back)

    serve(0)
    serve(1)
    serve(2)
    serve(3)
    pltpu.make_async_remote_copy(
        src_ref=results.at[(1 - core) * n_ep + me],
        dst_ref=returned.at[me * n_tp + core],
        send_sem=back_send,
        recv_sem=back_recv,
        device_id=(me, 1 - core),
        device_id_type=MESH,
    ).start()
    returned[me * n_tp + core] = results[core * n_ep + me]
    others = pl.ds(0, n_ep - 1)
    pltpu.make_async_copy(outgoing.at[others], outgoing.at[others], go_send).wait()
    others = pl.ds(0, n_ep * n_tp - 1)
    pltpu.make_async_copy(returned.at[others], returned.at[others], back_recv).wait()
    pltpu.make_async_copy(results.at[others], results.at[others], back_send).wait()
    fetched = returned[...].astype(F32).reshape(slots * n_tp, half).astype(BF16)
    down = (((0,), (0,)), ((), ()))
    blended = (
        base
        + lax.dot_general(upper, fetched, down, preferred_element_type=F32)
        + lax.dot_general(lower, fetched, down, preferred_element_type=F32)
    )
    total = jnp.sum(blended, axis=1, keepdims=True)
    squares = jnp.sum(blended * blended, axis=1, keepdims=True)
    lane = lax.broadcasted_iota(jnp.int32, stat_mine.shape, 1)
    stats = jnp.where(lane == 0, total, squares)
    stat_mine[...] = stats
    trade = pltpu.make_async_remote_copy(
        src_ref=stat_mine,
        dst_ref=stat_other,
        send_sem=stat_sem.at[0],
        recv_sem=stat_sem.at[1],
        device_id=(me, 1 - core),
        device_id_type=MESH,
    )
    trade.start()
    trade.wait()
    both = stats + stat_other[...]
    row_mean = both[:, 0:1] / width
    spread = both[:, 1:2] / width - row_mean * row_mean
    out_ref[...] = (
        (blended - row_mean) * lax.rsqrt(spread + eps_norm) * gain + shift
    ).astype(BF16)


def store_kernel(out_ref, fresh, out_hbm, new_hbm, out_sem, new_sem):
    for part in pieces(fresh.shape, fresh.dtype):
        pltpu.make_async_copy(fresh.at[part], new_hbm.at[part], new_sem).start()
    last = pltpu.make_async_copy(out_ref, out_hbm, out_sem)
    last.start()
    last.wait()
    pltpu.make_async_copy(fresh, new_hbm, new_sem).wait()


def on_device(
    n_ep,
    n_tp,
    tokens,
    recurrent_state,
    query_weight,
    key_weight,
    decay_weight,
    value_weight,
    gate_weight,
    head_gain,
    output_weight,
    norm_gain,
    norm_bias,
    group_router,
    router_weight,
    routes,
    expert_gate,
    expert_up,
    expert_down,
):
    rows, width = tokens.shape
    heads, key_dim, value_dim = recurrent_state.shape[1:]
    in_hbm = pl.BlockSpec(memory_space=pltpu.HBM)
    vmem = pl.BlockSpec(memory_space=pltpu.VMEM)
    chunk = 4
    chunks = rows // chunk
    dma = pltpu.SemaphoreType.DMA

    def like(a):
        return pltpu.VMEM(a.shape, a.dtype)

    def pinned(arrays):
        return tuple(pltpu.with_memory_space_constraint(a, pltpu.HBM) for a in arrays)

    experts = router_weight.shape[1]
    cap = 2 * max(1, rows // experts)
    half = width // n_tp
    operands = (
        tokens,
        recurrent_state,
        query_weight,
        key_weight,
        decay_weight,
        value_weight,
        gate_weight,
        head_gain.reshape(1, value_dim),
        output_weight,
        norm_gain,
        norm_bias,
        group_router.T,
        router_weight.T,
        routes.T,
        expert_gate,
        expert_up,
        expert_down,
    )
    new_tokens, new_state = pl.pallas_call(
        functools.partial(layer_kernel, n_ep, n_tp, cap, chunk),
        out_shape=(
            jax.ShapeDtypeStruct((rows, half), BF16),
            jax.ShapeDtypeStruct(recurrent_state.shape, F32),
        ),
        in_specs=[in_hbm] * len(operands),
        out_specs=(vmem, vmem),
        scratch_shapes=[like(a) for a in operands]
        + [
            pltpu.VMEM((rows, heads * value_dim), F32),
            pltpu.VMEM((rows, width), BF16),
            pltpu.VMEM((rows, width), BF16),
            pltpu.VMEM((n_ep, cap, width), BF16),
            pltpu.VMEM((n_ep, cap, width), BF16),
            pltpu.VMEM((n_tp * n_ep, cap, half), BF16),
            pltpu.VMEM((n_ep * n_tp, cap, half), BF16),
            pltpu.VMEM((rows, 128), F32),
            pltpu.VMEM((rows, 128), F32),
            dma((len(operands) - 1,)),
            dma((chunks,)),
            dma((2,)),
            dma((2,)),
            dma,
            dma((4,)),
            dma,
            dma,
        ],
        compiler_params=pltpu.CompilerParams(
            collective_id=0, has_side_effects=True, vmem_limit_bytes=40 * 1024 * 1024
        ),
        name="layer",
    )(*pinned(operands))
    return pl.pallas_call(
        store_kernel,
        out_shape=(
            jax.ShapeDtypeStruct(new_tokens.shape, BF16),
            jax.ShapeDtypeStruct(new_state.shape, F32),
        ),
        in_specs=[vmem, vmem],
        out_specs=(in_hbm, in_hbm),
        scratch_shapes=[dma, dma],
        compiler_params=pltpu.CompilerParams(vmem_limit_bytes=8 * 1024 * 1024),
        name="store",
    )(new_tokens, new_state)


def solution(mesh):
    in_specs = (
        P("ep", None),
        P("ep", "tp", None, None),
        P(None, "tp"),
        P(None, "tp"),
        P(None, "tp"),
        P(None, "tp"),
        P(None, "tp"),
        P(),
        P("tp", None),
        P(),
        P(),
        P(),
        P(),
        P("ep", None),
        P(("ep", "tp"), None, None),
        P(("ep", "tp"), None, None),
        P(("ep", "tp"), None, None),
    )
    out_specs = (P("ep", "tp"), P("ep", "tp", None, None))
    return jax.shard_map(
        functools.partial(on_device, mesh.shape["ep"], mesh.shape["tp"]),
        mesh=mesh,
        in_specs=in_specs,
        out_specs=out_specs,
        check_vma=False,
    )
```

```python
import functools
import math

import jax
import jax.numpy as jnp
from jax import lax
from jax.experimental import pallas as pl
from jax.experimental.pallas import tpu as pltpu
from jax.sharding import PartitionSpec as P

MESH = pl.DeviceIdType.MESH
alpha_res = 2.0**0.5
eps_norm = 1e-05
F32 = jnp.float32
BF16 = jnp.bfloat16
PIECE = 256 * 1024
AHEAD = 11 * 1024 * 1024


def dot32(a, b):
    return jnp.dot(a, b, preferred_element_type=F32)


def pieces(shape, dtype, size=PIECE):
    lead = 1 if len(shape) > 2 and shape[0] == 1 else 0
    whole = math.prod(shape) * jnp.dtype(dtype).itemsize
    count = max(1, min(whole // size, shape[lead] // (16 if len(shape) - lead == 2 else 1)))
    while shape[lead] % count:
        count -= 1
    step = shape[lead] // count
    return [(0,) * lead + (pl.ds(n * step, step),) for n in range(count)]


def layer_kernel(
    n_ep,
    n_tp,
    cap,
    chunk,
    tokens_hbm,
    state_hbm,
    wq_hbm,
    wk_hbm,
    wd_hbm,
    wv_hbm,
    wg_hbm,
    gain_hbm,
    wo_hbm,
    norm_gain_hbm,
    norm_bias_hbm,
    group_w_hbm,
    router_w_hbm,
    routes_hbm,
    eg_hbm,
    eu_hbm,
    ed_hbm,
    out_ref,
    fresh,
    tokens,
    state,
    wq,
    wk,
    wd,
    wv,
    wg,
    head_gain,
    wo,
    norm_gain,
    norm_bias,
    group_w,
    router_w,
    routes,
    eg,
    eu,
    ed,
    readout,
    part_mine,
    part_other,
    outgoing,
    arrived,
    results,
    returned,
    stat_mine,
    stat_other,
    in_sem,
    wo_sem,
    state_sem,
    pair_sem,
    stat_sem,
    go_send,
    go_recv,
    back_send,
    back_recv,
):
    me = lax.axis_index("ep")
    core = lax.axis_index("tp")
    rows, width = tokens.shape
    heads, key_dim, value_dim = state.shape[1:]
    half = width // n_tp
    per_group = router_w.shape[0] // group_w.shape[0]
    slots = n_ep * cap
    chunks = rows // chunk

    unrolled = n_ep <= 32 and n_ep & (n_ep - 1) == 0

    own_side = lax.div(me, n_ep // 2)

    def peer(i):
        if not unrolled:
            return lax.rem(me + i, n_ep)
        planes = n_ep // 4
        if i >= n_ep // 2 and planes > 1:
            plane = i // 4 + own_side * (planes - 1 - 2 * (i // 4))
            there = plane * 4 + lax.rem(me, 4)
            i = i % 4
        else:
            there = me
        bit = 1
        while bit < n_ep:
            if i & bit:
                there = there + bit * (1 - 2 * lax.rem(lax.div(me, bit), 2))
            bit *= 2
        return there

    order = sorted(range(1, n_ep), key=lambda i: -((i & 1) + (i >> 1 & 1) + (i >> 2)))

    def over_peers(body):
        if unrolled:
            for i in order:
                body(i)
        else:

            def step(i, carry):
                body(i)
                return carry

            lax.fori_loop(1, n_ep, step, 0)

    batches = ((0, 1), (1, n_ep // 4 - 1), (n_ep // 4, n_ep // 4), (n_ep // 2, n_ep // 2))
    own_batch = lax.div(me + n_ep - 1, n_ep) + lax.div(me, n_ep // 4) - lax.div(me, 3 * (n_ep // 4))

    names = (
        ("routes", routes_hbm, routes),
        ("tokens", tokens_hbm, tokens),
        ("wk", wk_hbm, wk),
        ("wd", wd_hbm, wd),
        ("wq", wq_hbm, wq),
        ("wv", wv_hbm, wv),
        ("wg", wg_hbm, wg),
        ("head_gain", gain_hbm, head_gain),
        ("norm_gain", norm_gain_hbm, norm_gain),
        ("norm_bias", norm_bias_hbm, norm_bias),
        ("group_w", group_w_hbm, group_w),
        ("router_w", router_w_hbm, router_w),
        ("eg", eg_hbm, eg),
        ("eu", eu_hbm, eu),
        ("ed", ed_hbm, ed),
    )
    load = {name: (src, dst, in_sem.at[n]) for n, (name, src, dst) in enumerate(names)}
    for c in range(n_tp):
        part = (slice(None), pl.ds(c * half, half))
        load["wo", c] = (wo_hbm.at[part], wo.at[part], wo_sem.at[c])
    for n in range(chunks):
        part = pl.ds(n * chunk, chunk)
        load[n] = (state_hbm.at[part], state.at[part], state_sem.at[n])

    def fetch(name, urgent):
        src, dst, sem = load[name]
        for part in pieces(src.shape, src.dtype):
            pltpu.make_async_copy(src.at[part], dst.at[part], sem).start(
                priority=0 if urgent else 1
            )

    def ready(name):
        pltpu.make_async_copy(*load[name]).wait()
        flying.pop(name)
        fetch_more()

    queue = [*("routes", "tokens", "wd", "wq"), *range(chunks), *("wk", "wv", "head_gain", "wg")]
    queue += [*(("wo", c) for c in range(n_tp)), "norm_gain", "norm_bias", "group_w", "router_w", "eg", "eu", "ed"]
    urgent = queue[: 4 + chunks]
    flying = {}

    def fetch_more():
        while queue and sum(flying.values()) < AHEAD:
            name = queue.pop(0)
            src = load[name][0]
            flying[name] = math.prod(src.shape) * jnp.dtype(src.dtype).itemsize
            fetch(name, name in urgent)

    fetch_more()

    barrier = pltpu.get_barrier_semaphore()

    def greet(i):
        for c in range(n_tp):
            pl.semaphore_signal(barrier, inc=1, device_id=(peer(i), c), device_id_type=MESH)

    over_peers(greet)
    for c in range(1, n_tp):
        pl.semaphore_signal(
            barrier, inc=1, device_id=(me, lax.rem(core + c, n_tp)), device_id_type=MESH
        )

    ready("routes")
    first, second = routes[0:1, :], routes[1:2, :]
    before = (
        lax.broadcasted_iota(jnp.int32, (rows, rows), 0)
        < lax.broadcasted_iota(jnp.int32, (rows, rows), 1)
    ).astype(BF16)

    def slot_of(count, to_expert):
        line = lax.broadcasted_iota(jnp.int32, (count, rows), 0)
        expert = to_expert(lax.div(line, cap))
        place = lax.rem(line, cap).astype(F32)
        hit0, hit1 = first == expert, second == expert
        either = jnp.where(hit0, 1.0, jnp.where(hit1, 1.0, 0.0))
        earlier = dot32(either.astype(BF16), before)
        placed = jnp.where(earlier == place, 1.0, 0.0)
        return jnp.where(hit0, placed, 0.0), jnp.where(hit1, placed, 0.0)

    send0, send1 = slot_of(slots, lambda j: j * n_tp + core)
    pick_send = (send0 + send1).astype(BF16)
    back0, back1 = slot_of(slots * n_tp, lambda j: j)

    ready("tokens")
    x = tokens[...]
    ready("wd")
    pre = dot32(x, wd[...])
    decay = jnp.exp((jnp.minimum(pre, 0.0) - jnp.log1p(jnp.exp(-jnp.abs(pre)))) / 16.0)
    ready("wq")
    queries = dot32(x, wq[...]) * key_dim ** (-0.5)
    decayed = queries * decay

    def as_columns(parts):
        pad = jnp.zeros((key_dim - len(parts) * rows, key_dim), F32)
        return [
            jnp.concatenate([p[:, h * key_dim : (h + 1) * key_dim] for p in parts] + [pad], axis=0).T
            for h in range(heads)
        ]

    reading = as_columns([decayed])
    for n in range(chunks):
        ready(n)
        for b in range(n * chunk, (n + 1) * chunk):
            for h in range(heads):
                readout[b : b + 1, h * value_dim : (h + 1) * value_dim] = jnp.sum(
                    reading[h][:, b : b + 1] * state[b, h], axis=0, keepdims=True
                )
    ready("wk")
    keys = dot32(x, wk[...])
    ready("wv")
    values = dot32(x, wv[...])
    both = queries * keys
    ready("wg")
    gate = dot32(x, wg[...])
    ready("head_gain")
    gated = []
    for h in range(heads):
        part = slice(h * value_dim, (h + 1) * value_dim)
        meet = jnp.sum(both[:, h * key_dim : (h + 1) * key_dim], axis=-1, keepdims=True)
        r = readout[:, part] + meet * values[:, part]
        scale = lax.rsqrt(jnp.mean(r * r, axis=-1, keepdims=True) + eps_norm)
        gated.append((r * scale * head_gain[...] * jax.nn.silu(gate[:, part])).astype(BF16))
    gated = jnp.concatenate(gated, axis=1)
    for c in range(n_tp):
        ready(("wo", c))
        part = slice(c * half, (c + 1) * half)
        part_mine[:, part] = dot32(gated, wo[:, part]).astype(BF16)

    pl.semaphore_wait(barrier, n_ep * n_tp - 1)
    swap = pltpu.make_async_remote_copy(
        src_ref=part_mine,
        dst_ref=part_other,
        send_sem=pair_sem.at[0],
        recv_sem=pair_sem.at[1],
        device_id=(me, 1 - core),
        device_id_type=MESH,
    )
    swap.start()
    for name in ("norm_gain", "norm_bias", "group_w", "router_w"):
        ready(name)
    base = alpha_res * tokens[...].astype(F32) + part_mine[...].astype(F32)
    swap.wait()
    mixed = base + part_other[...].astype(F32)
    centered = mixed - jnp.mean(mixed, axis=-1, keepdims=True)
    spread = jnp.mean(centered * centered, axis=-1, keepdims=True)
    hidden = (
        centered * lax.rsqrt(spread + eps_norm) * norm_gain[0:1, :] + norm_bias[0:1, :]
    ).astype(BF16)

    outgoing[...] = dot32(pick_send, hidden).reshape(n_ep, cap, width).astype(BF16)

    def dispatch(i):
        there = peer(i)
        return pltpu.make_async_remote_copy(
            src_ref=outgoing.at[there],
            dst_ref=arrived.at[me],
            send_sem=go_send,
            recv_sem=go_recv.at[own_batch],
            device_id=(there, core),
            device_id_type=MESH,
        )

    over_peers(lambda i: dispatch(i).start())
    arrived[me] = outgoing[me]

    @pl.when(me >= 0)
    def _():
        columns = as_columns([keys, decay])
        for b in range(rows):
            for h in range(heads):
                col = columns[h]
                v = values[b : b + 1, h * value_dim : (h + 1) * value_dim]
                fresh[b, h] = col[:, rows + b : rows + b + 1] * state[b, h] + col[:, b : b + 1] * v

    across = (((1,), (1,)), ((), ()))
    group_logit = lax.dot_general(group_w[...], hidden, across, preferred_element_type=F32)
    expert_logit = lax.dot_general(router_w[...], hidden, across, preferred_element_type=F32)
    own_group = lax.div(first, per_group)
    group_hit = own_group == lax.broadcasted_iota(jnp.int32, group_logit.shape, 0)
    own_logit = jnp.sum(jnp.where(group_hit, group_logit, 0.0), axis=0, keepdims=True)
    share = 1.0 / jnp.sum(jnp.exp(group_logit - own_logit), axis=0, keepdims=True)
    expert_iota = lax.broadcasted_iota(jnp.int32, expert_logit.shape, 0)
    logit0 = jnp.sum(jnp.where(first == expert_iota, expert_logit, 0.0), axis=0, keepdims=True)
    logit1 = jnp.sum(jnp.where(second == expert_iota, expert_logit, 0.0), axis=0, keepdims=True)
    weighted = back0 * (share * jax.nn.sigmoid(logit0 - logit1)) + back1 * (
        share * jax.nn.sigmoid(logit1 - logit0)
    )
    upper = weighted.astype(BF16)
    lower = (weighted - upper.astype(F32)).astype(BF16)
    mine = jnp.where(core == 0, hidden[:, :half].astype(F32), hidden[:, half:].astype(F32))
    base = alpha_res * mine
    gain = jnp.where(core == 0, norm_gain[1:2, :half], norm_gain[1:2, half:])
    shift = jnp.where(core == 0, norm_bias[1:2, :half], norm_bias[1:2, half:])
    for name in ("eg", "eu", "ed"):
        ready(name)

    def send_back(there, c):
        return pltpu.make_async_remote_copy(
            src_ref=results.at[c * n_ep + there],
            dst_ref=returned.at[me * n_tp + core],
            send_sem=back_send,
            recv_sem=back_recv,
            device_id=(there, c),
            device_id_type=MESH,
        )

    def landed(batch, count):
        some = arrived.at[pl.ds(0, count)]
        pltpu.make_async_copy(some, some, go_recv.at[batch]).wait()

    def serve(batch):
        start, size = batches[batch]
        if size > 1:
            pl.when(own_batch == batch)(lambda: landed(batch, size - 1))
        pl.when(own_batch != batch)(lambda: landed(batch, size))
        rows_in = arrived[start : start + size].astype(F32)
        rows_in = rows_in.reshape(size * cap, width).astype(BF16)
        gate_part = dot32(rows_in, eg[0])
        up_part = dot32(rows_in, eu[0])
        activation = (jax.nn.silu(gate_part) * up_part).astype(BF16)
        for c in range(n_tp):
            at = c * n_ep + start
            result = dot32(activation, ed[0, :, c * half : (c + 1) * half])
            results[at : at + size] = result.reshape(size, cap, half).astype(BF16)
            if size == 1:
                pl.when(own_batch != batch)(lambda: send_back(start, c).start())
                continue

            def back(i):
                there = peer(i)
                pl.when((there >= start) & (there < start + size))(lambda: send_back(there, c).start())

            over_peers(back)

    serve(0)
    serve(1)
    serve(2)
    serve(3)
    pltpu.make_async_remote_copy(
        src_ref=results.at[(1 - core) * n_ep + me],
        dst_ref=returned.at[me * n_tp + core],
        send_sem=back_send,
        recv_sem=back_recv,
        device_id=(me, 1 - core),
        device_id_type=MESH,
    ).start()
    returned[me * n_tp + core] = results[core * n_ep + me]
    others = pl.ds(0, n_ep - 1)
    pltpu.make_async_copy(outgoing.at[others], outgoing.at[others], go_send).wait()
    others = pl.ds(0, n_ep * n_tp - 1)
    pltpu.make_async_copy(returned.at[others], returned.at[others], back_recv).wait()
    pltpu.make_async_copy(results.at[others], results.at[others], back_send).wait()
    fetched = returned[...].astype(F32).reshape(slots * n_tp, half).astype(BF16)
    down = (((0,), (0,)), ((), ()))
    blended = (
        base
        + lax.dot_general(upper, fetched, down, preferred_element_type=F32)
        + lax.dot_general(lower, fetched, down, preferred_element_type=F32)
    )
    total = jnp.sum(blended, axis=1, keepdims=True)
    squares = jnp.sum(blended * blended, axis=1, keepdims=True)
    lane = lax.broadcasted_iota(jnp.int32, stat_mine.shape, 1)
    stats = jnp.where(lane == 0, total, squares)
    stat_mine[...] = stats
    trade = pltpu.make_async_remote_copy(
        src_ref=stat_mine,
        dst_ref=stat_other,
        send_sem=stat_sem.at[0],
        recv_sem=stat_sem.at[1],
        device_id=(me, 1 - core),
        device_id_type=MESH,
    )
    trade.start()
    trade.wait()
    both = stats + stat_other[...]
    row_mean = both[:, 0:1] / width
    spread = both[:, 1:2] / width - row_mean * row_mean
    out_ref[...] = (
        (blended - row_mean) * lax.rsqrt(spread + eps_norm) * gain + shift
    ).astype(BF16)


def store_kernel(out_ref, fresh, out_hbm, new_hbm, out_sem, new_sem):
    for part in pieces(fresh.shape, fresh.dtype):
        pltpu.make_async_copy(fresh.at[part], new_hbm.at[part], new_sem).start()
    last = pltpu.make_async_copy(out_ref, out_hbm, out_sem)
    last.start()
    last.wait()
    pltpu.make_async_copy(fresh, new_hbm, new_sem).wait()


def on_device(
    n_ep,
    n_tp,
    tokens,
    recurrent_state,
    query_weight,
    key_weight,
    decay_weight,
    value_weight,
    gate_weight,
    head_gain,
    output_weight,
    norm_gain,
    norm_bias,
    group_router,
    router_weight,
    routes,
    expert_gate,
    expert_up,
    expert_down,
):
    rows, width = tokens.shape
    heads, key_dim, value_dim = recurrent_state.shape[1:]
    in_hbm = pl.BlockSpec(memory_space=pltpu.HBM)
    vmem = pl.BlockSpec(memory_space=pltpu.VMEM)
    chunk = 4
    chunks = rows // chunk
    dma = pltpu.SemaphoreType.DMA

    def like(a):
        return pltpu.VMEM(a.shape, a.dtype)

    def pinned(arrays):
        return tuple(pltpu.with_memory_space_constraint(a, pltpu.HBM) for a in arrays)

    experts = router_weight.shape[1]
    cap = 2 * max(1, rows // experts)
    half = width // n_tp
    operands = (
        tokens,
        recurrent_state,
        query_weight,
        key_weight,
        decay_weight,
        value_weight,
        gate_weight,
        head_gain.reshape(1, value_dim),
        output_weight,
        norm_gain,
        norm_bias,
        group_router.T,
        router_weight.T,
        routes.T,
        expert_gate,
        expert_up,
        expert_down,
    )
    new_tokens, new_state = pl.pallas_call(
        functools.partial(layer_kernel, n_ep, n_tp, cap, chunk),
        out_shape=(
            jax.ShapeDtypeStruct((rows, half), BF16),
            jax.ShapeDtypeStruct(recurrent_state.shape, F32),
        ),
        in_specs=[in_hbm] * len(operands),
        out_specs=(vmem, vmem),
        scratch_shapes=[like(a) for a in operands]
        + [
            pltpu.VMEM((rows, heads * value_dim), F32),
            pltpu.VMEM((rows, width), BF16),
            pltpu.VMEM((rows, width), BF16),
            pltpu.VMEM((n_ep, cap, width), BF16),
            pltpu.VMEM((n_ep, cap, width), BF16),
            pltpu.VMEM((n_tp * n_ep, cap, half), BF16),
            pltpu.VMEM((n_ep * n_tp, cap, half), BF16),
            pltpu.VMEM((rows, 128), F32),
            pltpu.VMEM((rows, 128), F32),
            dma((len(operands) - 2,)),
            dma((n_tp,)),
            dma((chunks,)),
            dma((2,)),
            dma((2,)),
            dma,
            dma((4,)),
            dma,
            dma,
        ],
        compiler_params=pltpu.CompilerParams(
            collective_id=0, has_side_effects=True, vmem_limit_bytes=40 * 1024 * 1024
        ),
        name="layer",
    )(*pinned(operands))
    return pl.pallas_call(
        store_kernel,
        out_shape=(
            jax.ShapeDtypeStruct(new_tokens.shape, BF16),
            jax.ShapeDtypeStruct(new_state.shape, F32),
        ),
        in_specs=[vmem, vmem],
        out_specs=(in_hbm, in_hbm),
        scratch_shapes=[dma, dma],
        compiler_params=pltpu.CompilerParams(vmem_limit_bytes=8 * 1024 * 1024),
        name="store",
    )(new_tokens, new_state)


def solution(mesh):
    in_specs = (
        P("ep", None),
        P("ep", "tp", None, None),
        P(None, "tp"),
        P(None, "tp"),
        P(None, "tp"),
        P(None, "tp"),
        P(None, "tp"),
        P(),
        P("tp", None),
        P(),
        P(),
        P(),
        P(),
        P("ep", None),
        P(("ep", "tp"), None, None),
        P(("ep", "tp"), None, None),
        P(("ep", "tp"), None, None),
    )
    out_specs = (P("ep", "tp"), P("ep", "tp", None, None))
    return jax.shard_map(
        functools.partial(on_device, mesh.shape["ep"], mesh.shape["tp"]),
        mesh=mesh,
        in_specs=in_specs,
        out_specs=out_specs,
        check_vma=False,
    )
```

```python
import functools
import math

import jax
import jax.numpy as jnp
from jax import lax
from jax.experimental import pallas as pl
from jax.experimental.pallas import tpu as pltpu
from jax.sharding import PartitionSpec as P

MESH = pl.DeviceIdType.MESH
alpha_res = 2.0**0.5
eps_norm = 1e-05
F32 = jnp.float32
BF16 = jnp.bfloat16
PIECE = 256 * 1024
AHEAD = 11 * 1024 * 1024


def dot32(a, b):
    return jnp.dot(a, b, preferred_element_type=F32)


def pieces(shape, dtype, size=PIECE):
    lead = 1 if len(shape) > 2 and shape[0] == 1 else 0
    whole = math.prod(shape) * jnp.dtype(dtype).itemsize
    count = max(1, min(whole // size, shape[lead] // (16 if len(shape) - lead == 2 else 1)))
    while shape[lead] % count:
        count -= 1
    step = shape[lead] // count
    return [(0,) * lead + (pl.ds(n * step, step),) for n in range(count)]


def layer_kernel(
    n_ep,
    n_tp,
    cap,
    chunk,
    tokens_hbm,
    state_hbm,
    wq_hbm,
    wk_hbm,
    wd_hbm,
    wv_hbm,
    wg_hbm,
    gain_hbm,
    wo_hbm,
    norm_gain_hbm,
    norm_bias_hbm,
    group_w_hbm,
    router_w_hbm,
    routes_hbm,
    eg_hbm,
    eu_hbm,
    ed_hbm,
    out_ref,
    stat_ref,
    scale_ref,
    fresh,
    tokens,
    state,
    wq,
    wk,
    wd,
    wv,
    wg,
    head_gain,
    wo,
    norm_gain,
    norm_bias,
    group_w,
    router_w,
    routes,
    eg,
    eu,
    ed,
    readout,
    part_mine,
    part_other,
    outgoing,
    arrived,
    results,
    returned,
    stat_mine,
    stat_other,
    in_sem,
    wo_sem,
    state_sem,
    pair_sem,
    stat_sem,
    go_send,
    go_recv,
    back_send,
    back_recv,
):
    me = lax.axis_index("ep")
    core = lax.axis_index("tp")
    rows, width = tokens.shape
    heads, key_dim, value_dim = state.shape[1:]
    half = width // n_tp
    per_group = router_w.shape[0] // group_w.shape[0]
    slots = n_ep * cap
    chunks = rows // chunk

    unrolled = n_ep <= 32 and n_ep & (n_ep - 1) == 0

    own_side = lax.div(me, n_ep // 2)

    def peer(i):
        if not unrolled:
            return lax.rem(me + i, n_ep)
        planes = n_ep // 4
        if i >= n_ep // 2 and planes > 1:
            plane = i // 4 + own_side * (planes - 1 - 2 * (i // 4))
            there = plane * 4 + lax.rem(me, 4)
            i = i % 4
        else:
            there = me
        bit = 1
        while bit < n_ep:
            if i & bit:
                there = there + bit * (1 - 2 * lax.rem(lax.div(me, bit), 2))
            bit *= 2
        return there

    order = sorted(range(1, n_ep), key=lambda i: -((i & 1) + (i >> 1 & 1) + (i >> 2)))

    def over_peers(body):
        if unrolled:
            for i in order:
                body(i)
        else:

            def step(i, carry):
                body(i)
                return carry

            lax.fori_loop(1, n_ep, step, 0)

    batches = ((0, 1), (1, n_ep // 4 - 1), (n_ep // 4, n_ep // 4), (n_ep // 2, n_ep // 2))
    own_batch = lax.div(me + n_ep - 1, n_ep) + lax.div(me, n_ep // 4) - lax.div(me, 3 * (n_ep // 4))

    names = (
        ("routes", routes_hbm, routes),
        ("tokens", tokens_hbm, tokens),
        ("wk", wk_hbm, wk),
        ("wd", wd_hbm, wd),
        ("wq", wq_hbm, wq),
        ("wv", wv_hbm, wv),
        ("wg", wg_hbm, wg),
        ("head_gain", gain_hbm, head_gain),
        ("norm_gain", norm_gain_hbm, norm_gain),
        ("norm_bias", norm_bias_hbm, norm_bias),
        ("group_w", group_w_hbm, group_w),
        ("router_w", router_w_hbm, router_w),
        ("eg", eg_hbm, eg),
        ("eu", eu_hbm, eu),
        ("ed", ed_hbm, ed),
    )
    load = {name: (src, dst, in_sem.at[n]) for n, (name, src, dst) in enumerate(names)}
    for c in range(n_tp):
        part = (slice(None), pl.ds(c * half, half))
        load["wo", c] = (wo_hbm.at[part], wo.at[part], wo_sem.at[c])
    for n in range(chunks):
        part = pl.ds(n * chunk, chunk)
        load[n] = (state_hbm.at[part], state.at[part], state_sem.at[n])

    def fetch(name, urgent):
        src, dst, sem = load[name]
        for part in pieces(src.shape, src.dtype):
            pltpu.make_async_copy(src.at[part], dst.at[part], sem).start(
                priority=0 if urgent else 1
            )

    def ready(name):
        pltpu.make_async_copy(*load[name]).wait()
        flying.pop(name)
        fetch_more()

    queue = [*("routes", "tokens", "wd", "wq"), *range(chunks), *("wk", "wv", "head_gain", "wg")]
    queue += [*(("wo", c) for c in range(n_tp)), "norm_gain", "norm_bias", "group_w", "router_w", "eg", "eu", "ed"]
    urgent = queue[: 4 + chunks]
    flying = {}

    def fetch_more():
        while queue and sum(flying.values()) < AHEAD:
            name = queue.pop(0)
            src = load[name][0]
            flying[name] = math.prod(src.shape) * jnp.dtype(src.dtype).itemsize
            fetch(name, name in urgent)

    fetch_more()

    barrier = pltpu.get_barrier_semaphore()

    def greet(i):
        for c in range(n_tp):
            pl.semaphore_signal(barrier, inc=1, device_id=(peer(i), c), device_id_type=MESH)

    over_peers(greet)
    for c in range(1, n_tp):
        pl.semaphore_signal(
            barrier, inc=1, device_id=(me, lax.rem(core + c, n_tp)), device_id_type=MESH
        )

    ready("routes")
    first, second = routes[0:1, :], routes[1:2, :]
    before = (
        lax.broadcasted_iota(jnp.int32, (rows, rows), 0)
        < lax.broadcasted_iota(jnp.int32, (rows, rows), 1)
    ).astype(BF16)

    def slot_of(count, to_expert):
        line = lax.broadcasted_iota(jnp.int32, (count, rows), 0)
        expert = to_expert(lax.div(line, cap))
        place = lax.rem(line, cap).astype(F32)
        hit0, hit1 = first == expert, second == expert
        either = jnp.where(hit0, 1.0, jnp.where(hit1, 1.0, 0.0))
        earlier = dot32(either.astype(BF16), before)
        placed = jnp.where(earlier == place, 1.0, 0.0)
        return jnp.where(hit0, placed, 0.0), jnp.where(hit1, placed, 0.0)

    send0, send1 = slot_of(slots, lambda j: j * n_tp + core)
    pick_send = (send0 + send1).astype(BF16)
    back0, back1 = slot_of(slots * n_tp, lambda j: j)

    ready("tokens")
    x = tokens[...]
    ready("wd")
    pre = dot32(x, wd[...])
    decay = jnp.exp((jnp.minimum(pre, 0.0) - jnp.log1p(jnp.exp(-jnp.abs(pre)))) / 16.0)
    ready("wq")
    queries = dot32(x, wq[...]) * key_dim ** (-0.5)
    decayed = queries * decay

    def as_columns(parts):
        pad = jnp.zeros((key_dim - len(parts) * rows, key_dim), F32)
        return [
            jnp.concatenate([p[:, h * key_dim : (h + 1) * key_dim] for p in parts] + [pad], axis=0).T
            for h in range(heads)
        ]

    reading = as_columns([decayed])
    for n in range(chunks):
        ready(n)
        for b in range(n * chunk, (n + 1) * chunk):
            for h in range(heads):
                readout[b : b + 1, h * value_dim : (h + 1) * value_dim] = jnp.sum(
                    reading[h][:, b : b + 1] * state[b, h], axis=0, keepdims=True
                )
    ready("wk")
    keys = dot32(x, wk[...])
    ready("wv")
    values = dot32(x, wv[...])
    both = queries * keys
    ready("wg")
    gate = dot32(x, wg[...])
    ready("head_gain")
    gated = []
    for h in range(heads):
        part = slice(h * value_dim, (h + 1) * value_dim)
        meet = jnp.sum(both[:, h * key_dim : (h + 1) * key_dim], axis=-1, keepdims=True)
        r = readout[:, part] + meet * values[:, part]
        scale = lax.rsqrt(jnp.mean(r * r, axis=-1, keepdims=True) + eps_norm)
        gated.append((r * scale * head_gain[...] * jax.nn.silu(gate[:, part])).astype(BF16))
    gated = jnp.concatenate(gated, axis=1)
    for c in range(n_tp):
        ready(("wo", c))
        part = slice(c * half, (c + 1) * half)
        part_mine[:, part] = dot32(gated, wo[:, part]).astype(BF16)

    pl.semaphore_wait(barrier, n_ep * n_tp - 1)
    swap = pltpu.make_async_remote_copy(
        src_ref=part_mine,
        dst_ref=part_other,
        send_sem=pair_sem.at[0],
        recv_sem=pair_sem.at[1],
        device_id=(me, 1 - core),
        device_id_type=MESH,
    )
    swap.start()
    for name in ("norm_gain", "norm_bias", "group_w", "router_w"):
        ready(name)
    base = alpha_res * tokens[...].astype(F32) + part_mine[...].astype(F32)
    swap.wait()
    mixed = base + part_other[...].astype(F32)
    centered = mixed - jnp.mean(mixed, axis=-1, keepdims=True)
    spread = jnp.mean(centered * centered, axis=-1, keepdims=True)
    hidden = (
        centered * lax.rsqrt(spread + eps_norm) * norm_gain[0:1, :] + norm_bias[0:1, :]
    ).astype(BF16)

    outgoing[...] = dot32(pick_send, hidden).reshape(n_ep, cap, width).astype(BF16)

    def dispatch(i):
        there = peer(i)
        return pltpu.make_async_remote_copy(
            src_ref=outgoing.at[there],
            dst_ref=arrived.at[me],
            send_sem=go_send,
            recv_sem=go_recv.at[own_batch],
            device_id=(there, core),
            device_id_type=MESH,
        )

    over_peers(lambda i: dispatch(i).start())
    arrived[me] = outgoing[me]

    @pl.when(me >= 0)
    def _():
        columns = as_columns([keys, decay])
        for b in range(rows):
            for h in range(heads):
                col = columns[h]
                v = values[b : b + 1, h * value_dim : (h + 1) * value_dim]
                fresh[b, h] = col[:, rows + b : rows + b + 1] * state[b, h] + col[:, b : b + 1] * v

    across = (((1,), (1,)), ((), ()))
    group_logit = lax.dot_general(group_w[...], hidden, across, preferred_element_type=F32)
    expert_logit = lax.dot_general(router_w[...], hidden, across, preferred_element_type=F32)
    own_group = lax.div(first, per_group)
    group_hit = own_group == lax.broadcasted_iota(jnp.int32, group_logit.shape, 0)
    own_logit = jnp.sum(jnp.where(group_hit, group_logit, 0.0), axis=0, keepdims=True)
    share = 1.0 / jnp.sum(jnp.exp(group_logit - own_logit), axis=0, keepdims=True)
    expert_iota = lax.broadcasted_iota(jnp.int32, expert_logit.shape, 0)
    logit0 = jnp.sum(jnp.where(first == expert_iota, expert_logit, 0.0), axis=0, keepdims=True)
    logit1 = jnp.sum(jnp.where(second == expert_iota, expert_logit, 0.0), axis=0, keepdims=True)
    weighted = back0 * (share * jax.nn.sigmoid(logit0 - logit1)) + back1 * (
        share * jax.nn.sigmoid(logit1 - logit0)
    )
    upper = weighted.astype(BF16)
    lower = (weighted - upper.astype(F32)).astype(BF16)
    mine = jnp.where(core == 0, hidden[:, :half].astype(F32), hidden[:, half:].astype(F32))
    base = alpha_res * mine
    gain = jnp.where(core == 0, norm_gain[1:2, :half], norm_gain[1:2, half:])
    shift = jnp.where(core == 0, norm_bias[1:2, :half], norm_bias[1:2, half:])
    for name in ("eg", "eu", "ed"):
        ready(name)

    def send_back(there, c):
        return pltpu.make_async_remote_copy(
            src_ref=results.at[c * n_ep + there],
            dst_ref=returned.at[me * n_tp + core],
            send_sem=back_send,
            recv_sem=back_recv,
            device_id=(there, c),
            device_id_type=MESH,
        )

    def landed(batch, count):
        some = arrived.at[pl.ds(0, count)]
        pltpu.make_async_copy(some, some, go_recv.at[batch]).wait()

    def serve(batch):
        start, size = batches[batch]
        if size > 1:
            pl.when(own_batch == batch)(lambda: landed(batch, size - 1))
        pl.when(own_batch != batch)(lambda: landed(batch, size))
        rows_in = arrived[start : start + size].astype(F32)
        rows_in = rows_in.reshape(size * cap, width).astype(BF16)
        gate_part = dot32(rows_in, eg[0])
        up_part = dot32(rows_in, eu[0])
        activation = (jax.nn.silu(gate_part) * up_part).astype(BF16)
        for c in range(n_tp):
            at = c * n_ep + start
            result = dot32(activation, ed[0, :, c * half : (c + 1) * half])
            results[at : at + size] = result.reshape(size, cap, half).astype(BF16)
            if size == 1:
                pl.when(own_batch != batch)(lambda: send_back(start, c).start())
                continue

            def back(i):
                there = peer(i)
                pl.when((there >= start) & (there < start + size))(lambda: send_back(there, c).start())

            over_peers(back)

    serve(0)
    serve(1)
    serve(2)
    serve(3)
    pltpu.make_async_remote_copy(
        src_ref=results.at[(1 - core) * n_ep + me],
        dst_ref=returned.at[me * n_tp + core],
        send_sem=back_send,
        recv_sem=back_recv,
        device_id=(me, 1 - core),
        device_id_type=MESH,
    ).start()
    returned[me * n_tp + core] = results[core * n_ep + me]
    others = pl.ds(0, n_ep - 1)
    pltpu.make_async_copy(outgoing.at[others], outgoing.at[others], go_send).wait()
    others = pl.ds(0, n_ep * n_tp - 1)
    pltpu.make_async_copy(returned.at[others], returned.at[others], back_recv).wait()
    pltpu.make_async_copy(results.at[others], results.at[others], back_send).wait()
    fetched = returned[...].astype(F32).reshape(slots * n_tp, half).astype(BF16)
    down = (((0,), (0,)), ((), ()))
    blended = (
        base
        + lax.dot_general(upper, fetched, down, preferred_element_type=F32)
        + lax.dot_general(lower, fetched, down, preferred_element_type=F32)
    )
    total = jnp.sum(blended, axis=1, keepdims=True)
    squares = jnp.sum(blended * blended, axis=1, keepdims=True)
    lane = lax.broadcasted_iota(jnp.int32, stat_mine.shape, 1)
    stats = jnp.where(lane == 0, total, squares)
    stat_mine[...] = stats
    out_ref[...] = blended
    scale_ref[0:1, :] = gain
    scale_ref[1:2, :] = shift
    trade = pltpu.make_async_remote_copy(
        src_ref=stat_mine,
        dst_ref=stat_other,
        send_sem=stat_sem.at[0],
        recv_sem=stat_sem.at[1],
        device_id=(me, 1 - core),
        device_id_type=MESH,
    )
    trade.start()
    trade.wait()
    stat_ref[...] = stats + stat_other[...]


def store_kernel(width, blended, stats, scale, fresh, out_hbm, new_hbm, out, out_sem, new_sem):
    for part in pieces(fresh.shape, fresh.dtype):
        pltpu.make_async_copy(fresh.at[part], new_hbm.at[part], new_sem).start()
    row_mean = stats[:, 0:1] / width
    spread = stats[:, 1:2] / width - row_mean * row_mean
    out[...] = (
        (blended[...] - row_mean) * lax.rsqrt(spread + eps_norm) * scale[0:1, :] + scale[1:2, :]
    ).astype(BF16)
    last = pltpu.make_async_copy(out, out_hbm, out_sem)
    last.start()
    last.wait()
    pltpu.make_async_copy(fresh, new_hbm, new_sem).wait()


def on_device(
    n_ep,
    n_tp,
    tokens,
    recurrent_state,
    query_weight,
    key_weight,
    decay_weight,
    value_weight,
    gate_weight,
    head_gain,
    output_weight,
    norm_gain,
    norm_bias,
    group_router,
    router_weight,
    routes,
    expert_gate,
    expert_up,
    expert_down,
):
    rows, width = tokens.shape
    heads, key_dim, value_dim = recurrent_state.shape[1:]
    in_hbm = pl.BlockSpec(memory_space=pltpu.HBM)
    vmem = pl.BlockSpec(memory_space=pltpu.VMEM)
    chunk = 4
    chunks = rows // chunk
    dma = pltpu.SemaphoreType.DMA

    def like(a):
        return pltpu.VMEM(a.shape, a.dtype)

    def pinned(arrays):
        return tuple(pltpu.with_memory_space_constraint(a, pltpu.HBM) for a in arrays)

    experts = router_weight.shape[1]
    cap = 2 * max(1, rows // experts)
    half = width // n_tp
    operands = (
        tokens,
        recurrent_state,
        query_weight,
        key_weight,
        decay_weight,
        value_weight,
        gate_weight,
        head_gain.reshape(1, value_dim),
        output_weight,
        norm_gain,
        norm_bias,
        group_router.T,
        router_weight.T,
        routes.T,
        expert_gate,
        expert_up,
        expert_down,
    )
    blended, stats, scale, fresh = pl.pallas_call(
        functools.partial(layer_kernel, n_ep, n_tp, cap, chunk),
        out_shape=(
            jax.ShapeDtypeStruct((rows, half), F32),
            jax.ShapeDtypeStruct((rows, 128), F32),
            jax.ShapeDtypeStruct((2, half), F32),
            jax.ShapeDtypeStruct(recurrent_state.shape, F32),
        ),
        in_specs=[in_hbm] * len(operands),
        out_specs=(vmem,) * 4,
        scratch_shapes=[like(a) for a in operands]
        + [
            pltpu.VMEM((rows, heads * value_dim), F32),
            pltpu.VMEM((rows, width), BF16),
            pltpu.VMEM((rows, width), BF16),
            pltpu.VMEM((n_ep, cap, width), BF16),
            pltpu.VMEM((n_ep, cap, width), BF16),
            pltpu.VMEM((n_tp * n_ep, cap, half), BF16),
            pltpu.VMEM((n_ep * n_tp, cap, half), BF16),
            pltpu.VMEM((rows, 128), F32),
            pltpu.VMEM((rows, 128), F32),
            dma((len(operands) - 2,)),
            dma((n_tp,)),
            dma((chunks,)),
            dma((2,)),
            dma((2,)),
            dma,
            dma((4,)),
            dma,
            dma,
        ],
        compiler_params=pltpu.CompilerParams(
            collective_id=0, has_side_effects=True, vmem_limit_bytes=40 * 1024 * 1024
        ),
        name="layer",
    )(*pinned(operands))
    return pl.pallas_call(
        functools.partial(store_kernel, width),
        out_shape=(
            jax.ShapeDtypeStruct((rows, half), BF16),
            jax.ShapeDtypeStruct(fresh.shape, F32),
        ),
        in_specs=[vmem] * 4,
        out_specs=(in_hbm, in_hbm),
        scratch_shapes=[pltpu.VMEM((rows, half), BF16), dma, dma],
        compiler_params=pltpu.CompilerParams(vmem_limit_bytes=8 * 1024 * 1024),
        name="store",
    )(blended, stats, scale, fresh)


def solution(mesh):
    in_specs = (
        P("ep", None),
        P("ep", "tp", None, None),
        P(None, "tp"),
        P(None, "tp"),
        P(None, "tp"),
        P(None, "tp"),
        P(None, "tp"),
        P(),
        P("tp", None),
        P(),
        P(),
        P(),
        P(),
        P("ep", None),
        P(("ep", "tp"), None, None),
        P(("ep", "tp"), None, None),
        P(("ep", "tp"), None, None),
    )
    out_specs = (P("ep", "tp"), P("ep", "tp", None, None))
    return jax.shard_map(
        functools.partial(on_device, mesh.shape["ep"], mesh.shape["tp"]),
        mesh=mesh,
        in_specs=in_specs,
        out_specs=out_specs,
        check_vma=False,
    )
```

```python
import functools
import math

import jax
import jax.numpy as jnp
from jax import lax
from jax.experimental import pallas as pl
from jax.experimental.pallas import tpu as pltpu
from jax.sharding import PartitionSpec as P

MESH = pl.DeviceIdType.MESH
alpha_res = 2.0**0.5
eps_norm = 1e-05
F32 = jnp.float32
BF16 = jnp.bfloat16
PIECE = 256 * 1024
AHEAD = 11 * 1024 * 1024


def dot32(a, b):
    return jnp.dot(a, b, preferred_element_type=F32)


def pieces(shape, dtype, size=PIECE):
    lead = 1 if len(shape) > 2 and shape[0] == 1 else 0
    whole = math.prod(shape) * jnp.dtype(dtype).itemsize
    count = max(1, min(whole // size, shape[lead] // (16 if len(shape) - lead == 2 else 1)))
    while shape[lead] % count:
        count -= 1
    step = shape[lead] // count
    return [(0,) * lead + (pl.ds(n * step, step),) for n in range(count)]


def layer_kernel(
    n_ep,
    n_tp,
    cap,
    chunk,
    tokens_hbm,
    state_hbm,
    wq_hbm,
    wk_hbm,
    wd_hbm,
    wv_hbm,
    wg_hbm,
    gain_hbm,
    wo_hbm,
    norm_gain_hbm,
    norm_bias_hbm,
    group_w_hbm,
    router_w_hbm,
    routes_hbm,
    eg_hbm,
    eu_hbm,
    ed_hbm,
    out_ref,
    stat_ref,
    scale_ref,
    fresh,
    tokens,
    state,
    wq,
    wk,
    wd,
    wv,
    wg,
    head_gain,
    wo,
    norm_gain,
    norm_bias,
    group_w,
    router_w,
    routes,
    eg,
    eu,
    ed,
    readout,
    part_mine,
    part_other,
    outgoing,
    arrived,
    results,
    returned,
    stat_mine,
    stat_other,
    in_sem,
    wo_sem,
    state_sem,
    pair_sem,
    stat_sem,
    go_send,
    go_recv,
    back_send,
    back_recv,
):
    me = lax.axis_index("ep")
    core = lax.axis_index("tp")
    rows, width = tokens.shape
    heads, key_dim, value_dim = state.shape[1:]
    half = width // n_tp
    per_group = router_w.shape[0] // group_w.shape[0]
    slots = n_ep * cap
    chunks = rows // chunk

    unrolled = n_ep <= 32 and n_ep & (n_ep - 1) == 0

    own_side = lax.div(me, n_ep // 2)

    def peer(i):
        if not unrolled:
            return lax.rem(me + i, n_ep)
        planes = n_ep // 4
        if i >= n_ep // 2 and planes > 1:
            plane = i // 4 + own_side * (planes - 1 - 2 * (i // 4))
            there = plane * 4 + lax.rem(me, 4)
            i = i % 4
        else:
            there = me
        bit = 1
        while bit < n_ep:
            if i & bit:
                there = there + bit * (1 - 2 * lax.rem(lax.div(me, bit), 2))
            bit *= 2
        return there

    order = sorted(range(1, n_ep), key=lambda i: -((i & 1) + (i >> 1 & 1) + (i >> 2)))

    def over_peers(body):
        if unrolled:
            for i in order:
                body(i)
        else:

            def step(i, carry):
                body(i)
                return carry

            lax.fori_loop(1, n_ep, step, 0)

    batches = ((0, 1), (1, n_ep // 4 - 1), (n_ep // 4, n_ep // 4), (n_ep // 2, n_ep // 2))
    own_batch = lax.div(me + n_ep - 1, n_ep) + lax.div(me, n_ep // 4) - lax.div(me, 3 * (n_ep // 4))

    names = (
        ("routes", routes_hbm, routes),
        ("tokens", tokens_hbm, tokens),
        ("wk", wk_hbm, wk),
        ("wd", wd_hbm, wd),
        ("wq", wq_hbm, wq),
        ("wv", wv_hbm, wv),
        ("wg", wg_hbm, wg),
        ("head_gain", gain_hbm, head_gain),
        ("norm_gain", norm_gain_hbm, norm_gain),
        ("norm_bias", norm_bias_hbm, norm_bias),
        ("group_w", group_w_hbm, group_w),
        ("router_w", router_w_hbm, router_w),
        ("eg", eg_hbm, eg),
        ("eu", eu_hbm, eu),
        ("ed", ed_hbm, ed),
    )
    load = {name: (src, dst, in_sem.at[n]) for n, (name, src, dst) in enumerate(names)}
    for c in range(n_tp):
        part = (slice(None), pl.ds(c * half, half))
        load["wo", c] = (wo_hbm.at[part], wo.at[part], wo_sem.at[c])
    for n in range(chunks):
        part = pl.ds(n * chunk, chunk)
        load[n] = (state_hbm.at[part], state.at[part], state_sem.at[n])

    def fetch(name, urgent):
        src, dst, sem = load[name]
        for part in pieces(src.shape, src.dtype):
            pltpu.make_async_copy(src.at[part], dst.at[part], sem).start(
                priority=0 if urgent else 1
            )

    def ready(name):
        pltpu.make_async_copy(*load[name]).wait()
        flying.pop(name)
        fetch_more()

    queue = [*("routes", "tokens", "wd", "wq"), *range(chunks), *("wk", "wv", "head_gain", "wg")]
    queue += [*(("wo", c) for c in range(n_tp)), "norm_gain", "norm_bias", "group_w", "router_w", "eg", "eu", "ed"]
    urgent = queue[: 4 + chunks]
    flying = {}

    def fetch_more():
        while queue and sum(flying.values()) < AHEAD:
            name = queue.pop(0)
            src = load[name][0]
            flying[name] = math.prod(src.shape) * jnp.dtype(src.dtype).itemsize
            fetch(name, name in urgent)

    fetch_more()

    barrier = pltpu.get_barrier_semaphore()

    def greet(i):
        for c in range(n_tp):
            pl.semaphore_signal(barrier, inc=1, device_id=(peer(i), c), device_id_type=MESH)

    over_peers(greet)
    for c in range(1, n_tp):
        pl.semaphore_signal(
            barrier, inc=1, device_id=(me, lax.rem(core + c, n_tp)), device_id_type=MESH
        )

    ready("routes")
    first, second = routes[0:1, :], routes[1:2, :]
    before = (
        lax.broadcasted_iota(jnp.int32, (rows, rows), 0)
        < lax.broadcasted_iota(jnp.int32, (rows, rows), 1)
    ).astype(BF16)

    def slot_of(count, to_expert):
        line = lax.broadcasted_iota(jnp.int32, (count, rows), 0)
        expert = to_expert(lax.div(line, cap))
        place = lax.rem(line, cap).astype(F32)
        hit0, hit1 = first == expert, second == expert
        either = jnp.where(hit0, 1.0, jnp.where(hit1, 1.0, 0.0))
        earlier = dot32(either.astype(BF16), before)
        placed = jnp.where(earlier == place, 1.0, 0.0)
        return jnp.where(hit0, placed, 0.0), jnp.where(hit1, placed, 0.0)

    send0, send1 = slot_of(slots, lambda j: j * n_tp + core)
    pick_send = (send0 + send1).astype(BF16)
    back0, back1 = slot_of(slots * n_tp, lambda j: j)

    ready("tokens")
    x = tokens[...]
    ready("wd")
    pre = dot32(x, wd[...])
    decay = jnp.exp((jnp.minimum(pre, 0.0) - jnp.log1p(jnp.exp(-jnp.abs(pre)))) / 16.0)
    ready("wq")
    queries = dot32(x, wq[...]) * key_dim ** (-0.5)
    decayed = queries * decay

    def as_columns(parts):
        pad = jnp.zeros((key_dim - len(parts) * rows, key_dim), F32)
        return [
            jnp.concatenate([p[:, h * key_dim : (h + 1) * key_dim] for p in parts] + [pad], axis=0).T
            for h in range(heads)
        ]

    reading = as_columns([decayed])
    for n in range(chunks):
        ready(n)
        for b in range(n * chunk, (n + 1) * chunk):
            for h in range(heads):
                readout[b : b + 1, h * value_dim : (h + 1) * value_dim] = jnp.sum(
                    reading[h][:, b : b + 1] * state[b, h], axis=0, keepdims=True
                )
    ready("wk")
    keys = dot32(x, wk[...])
    ready("wv")
    values = dot32(x, wv[...])
    both = queries * keys
    ready("wg")
    gate = dot32(x, wg[...])
    ready("head_gain")
    gated = []
    for h in range(heads):
        part = slice(h * value_dim, (h + 1) * value_dim)
        meet = jnp.sum(both[:, h * key_dim : (h + 1) * key_dim], axis=-1, keepdims=True)
        r = readout[:, part] + meet * values[:, part]
        scale = lax.rsqrt(jnp.mean(r * r, axis=-1, keepdims=True) + eps_norm)
        gated.append((r * scale * head_gain[...] * jax.nn.silu(gate[:, part])).astype(BF16))
    gated = jnp.concatenate(gated, axis=1)
    for c in range(n_tp):
        ready(("wo", c))
        part = slice(c * half, (c + 1) * half)
        part_mine[:, part] = dot32(gated, wo[:, part]).astype(BF16)

    pl.semaphore_wait(barrier, n_ep * n_tp - 1)
    swap = pltpu.make_async_remote_copy(
        src_ref=part_mine,
        dst_ref=part_other,
        send_sem=pair_sem.at[0],
        recv_sem=pair_sem.at[1],
        device_id=(me, 1 - core),
        device_id_type=MESH,
    )
    swap.start()
    for name in ("norm_gain", "norm_bias", "group_w", "router_w"):
        ready(name)
    base = alpha_res * tokens[...].astype(F32) + part_mine[...].astype(F32)
    swap.wait()
    mixed = base + part_other[...].astype(F32)
    centered = mixed - jnp.mean(mixed, axis=-1, keepdims=True)
    spread = jnp.mean(centered * centered, axis=-1, keepdims=True)
    hidden = (
        centered * lax.rsqrt(spread + eps_norm) * norm_gain[0:1, :] + norm_bias[0:1, :]
    ).astype(BF16)

    outgoing[...] = dot32(pick_send, hidden).reshape(n_ep, cap, width).astype(BF16)

    def dispatch(i):
        there = peer(i)
        return pltpu.make_async_remote_copy(
            src_ref=outgoing.at[there],
            dst_ref=arrived.at[me],
            send_sem=go_send,
            recv_sem=go_recv.at[own_batch],
            device_id=(there, core),
            device_id_type=MESH,
        )

    over_peers(lambda i: dispatch(i).start())
    arrived[me] = outgoing[me]

    @pl.when(me >= 0)
    def _():
        columns = as_columns([keys, decay])
        for b in range(rows):
            for h in range(heads):
                col = columns[h]
                v = values[b : b + 1, h * value_dim : (h + 1) * value_dim]
                fresh[b, h] = col[:, rows + b : rows + b + 1] * state[b, h] + col[:, b : b + 1] * v

    across = (((1,), (1,)), ((), ()))
    group_logit = lax.dot_general(group_w[...], hidden, across, preferred_element_type=F32)
    expert_logit = lax.dot_general(router_w[...], hidden, across, preferred_element_type=F32)
    own_group = lax.div(first, per_group)
    group_hit = own_group == lax.broadcasted_iota(jnp.int32, group_logit.shape, 0)
    own_logit = jnp.sum(jnp.where(group_hit, group_logit, 0.0), axis=0, keepdims=True)
    share = 1.0 / jnp.sum(jnp.exp(group_logit - own_logit), axis=0, keepdims=True)
    expert_iota = lax.broadcasted_iota(jnp.int32, expert_logit.shape, 0)
    logit0 = jnp.sum(jnp.where(first == expert_iota, expert_logit, 0.0), axis=0, keepdims=True)
    logit1 = jnp.sum(jnp.where(second == expert_iota, expert_logit, 0.0), axis=0, keepdims=True)
    weighted = back0 * (share * jax.nn.sigmoid(logit0 - logit1)) + back1 * (
        share * jax.nn.sigmoid(logit1 - logit0)
    )
    upper = weighted.astype(BF16)
    lower = (weighted - upper.astype(F32)).astype(BF16)
    mine = jnp.where(core == 0, hidden[:, :half].astype(F32), hidden[:, half:].astype(F32))
    base = alpha_res * mine
    gain = jnp.where(core == 0, norm_gain[1:2, :half], norm_gain[1:2, half:])
    shift = jnp.where(core == 0, norm_bias[1:2, :half], norm_bias[1:2, half:])
    for name in ("eg", "eu", "ed"):
        ready(name)

    def send_back(there, c):
        return pltpu.make_async_remote_copy(
            src_ref=results.at[c * n_ep + there],
            dst_ref=returned.at[me * n_tp + core],
            send_sem=back_send,
            recv_sem=back_recv,
            device_id=(there, c),
            device_id_type=MESH,
        )

    def landed(batch, count):
        some = arrived.at[pl.ds(0, count)]
        pltpu.make_async_copy(some, some, go_recv.at[batch]).wait()

    def serve(batch):
        start, size = batches[batch]
        if size > 1:
            pl.when(own_batch == batch)(lambda: landed(batch, size - 1))
        pl.when(own_batch != batch)(lambda: landed(batch, size))
        rows_in = arrived[start : start + size].astype(F32)
        rows_in = rows_in.reshape(size * cap, width).astype(BF16)
        gate_part = dot32(rows_in, eg[0])
        up_part = dot32(rows_in, eu[0])
        activation = (jax.nn.silu(gate_part) * up_part).astype(BF16)
        for c in range(n_tp):
            at = c * n_ep + start
            result = dot32(activation, ed[0, :, c * half : (c + 1) * half])
            results[at : at + size] = result.reshape(size, cap, half).astype(BF16)
            if size == 1:
                pl.when(own_batch != batch)(lambda: send_back(start, c).start())
                continue

            def back(i):
                there = peer(i)
                pl.when((there >= start) & (there < start + size))(lambda: send_back(there, c).start())

            over_peers(back)

    serve(0)
    serve(1)
    serve(2)
    serve(3)
    pltpu.make_async_remote_copy(
        src_ref=results.at[(1 - core) * n_ep + me],
        dst_ref=returned.at[me * n_tp + core],
        send_sem=back_send,
        recv_sem=back_recv,
        device_id=(me, 1 - core),
        device_id_type=MESH,
    ).start()
    returned[me * n_tp + core] = results[core * n_ep + me]
    others = pl.ds(0, n_ep - 1)
    pltpu.make_async_copy(outgoing.at[others], outgoing.at[others], go_send).wait()
    others = pl.ds(0, n_ep * n_tp - 1)
    pltpu.make_async_copy(returned.at[others], returned.at[others], back_recv).wait()
    pltpu.make_async_copy(results.at[others], results.at[others], back_send).wait()
    fetched = returned[...].astype(F32).reshape(slots * n_tp, half).astype(BF16)
    down = (((0,), (0,)), ((), ()))
    blended = (
        base
        + lax.dot_general(upper, fetched, down, preferred_element_type=F32)
        + lax.dot_general(lower, fetched, down, preferred_element_type=F32)
    )
    total = jnp.sum(blended, axis=1, keepdims=True)
    squares = jnp.sum(blended * blended, axis=1, keepdims=True)
    lane = lax.broadcasted_iota(jnp.int32, stat_mine.shape, 1)
    stats = jnp.where(lane == 0, total, squares)
    stat_mine[...] = stats
    out_ref[...] = blended
    scale_ref[0:1, :] = gain
    scale_ref[1:2, :] = shift
    trade = pltpu.make_async_remote_copy(
        src_ref=stat_mine,
        dst_ref=stat_other,
        send_sem=stat_sem.at[0],
        recv_sem=stat_sem.at[1],
        device_id=(me, 1 - core),
        device_id_type=MESH,
    )
    trade.start()
    trade.wait()
    stat_ref[...] = stats + stat_other[...]


def store_kernel(width, blended, stats, scale, fresh, out_hbm, new_hbm, out, out_sem, new_sem):
    for part in pieces(fresh.shape, fresh.dtype):
        pltpu.make_async_copy(fresh.at[part], new_hbm.at[part], new_sem).start()
    row_mean = stats[:, 0:1] / width
    spread = stats[:, 1:2] / width - row_mean * row_mean
    out[...] = (
        (blended[...] - row_mean) * lax.rsqrt(spread + eps_norm) * scale[0:1, :] + scale[1:2, :]
    ).astype(BF16)
    last = pltpu.make_async_copy(out, out_hbm, out_sem)
    last.start()
    last.wait()
    pltpu.make_async_copy(fresh, new_hbm, new_sem).wait()


def on_device(
    n_ep,
    n_tp,
    tokens,
    recurrent_state,
    query_weight,
    key_weight,
    decay_weight,
    value_weight,
    gate_weight,
    head_gain,
    output_weight,
    norm_gain,
    norm_bias,
    group_router,
    router_weight,
    routes,
    expert_gate,
    expert_up,
    expert_down,
):
    rows, width = tokens.shape
    heads, key_dim, value_dim = recurrent_state.shape[1:]
    in_hbm = pl.BlockSpec(memory_space=pltpu.HBM)
    vmem = pl.BlockSpec(memory_space=pltpu.VMEM)
    chunk = 8
    chunks = rows // chunk
    dma = pltpu.SemaphoreType.DMA

    def like(a):
        return pltpu.VMEM(a.shape, a.dtype)

    def pinned(arrays):
        return tuple(pltpu.with_memory_space_constraint(a, pltpu.HBM) for a in arrays)

    experts = router_weight.shape[1]
    cap = 2 * max(1, rows // experts)
    half = width // n_tp
    operands = (
        tokens,
        recurrent_state,
        query_weight,
        key_weight,
        decay_weight,
        value_weight,
        gate_weight,
        head_gain.reshape(1, value_dim),
        output_weight,
        norm_gain,
        norm_bias,
        group_router.T,
        router_weight.T,
        routes.T,
        expert_gate,
        expert_up,
        expert_down,
    )
    blended, stats, scale, fresh = pl.pallas_call(
        functools.partial(layer_kernel, n_ep, n_tp, cap, chunk),
        out_shape=(
            jax.ShapeDtypeStruct((rows, half), F32),
            jax.ShapeDtypeStruct((rows, 128), F32),
            jax.ShapeDtypeStruct((2, half), F32),
            jax.ShapeDtypeStruct(recurrent_state.shape, F32),
        ),
        in_specs=[in_hbm] * len(operands),
        out_specs=(vmem,) * 4,
        scratch_shapes=[like(a) for a in operands]
        + [
            pltpu.VMEM((rows, heads * value_dim), F32),
            pltpu.VMEM((rows, width), BF16),
            pltpu.VMEM((rows, width), BF16),
            pltpu.VMEM((n_ep, cap, width), BF16),
            pltpu.VMEM((n_ep, cap, width), BF16),
            pltpu.VMEM((n_tp * n_ep, cap, half), BF16),
            pltpu.VMEM((n_ep * n_tp, cap, half), BF16),
            pltpu.VMEM((rows, 128), F32),
            pltpu.VMEM((rows, 128), F32),
            dma((len(operands) - 2,)),
            dma((n_tp,)),
            dma((chunks,)),
            dma((2,)),
            dma((2,)),
            dma,
            dma((4,)),
            dma,
            dma,
        ],
        compiler_params=pltpu.CompilerParams(
            collective_id=0, has_side_effects=True, vmem_limit_bytes=40 * 1024 * 1024
        ),
        name="layer",
    )(*pinned(operands))
    return pl.pallas_call(
        functools.partial(store_kernel, width),
        out_shape=(
            jax.ShapeDtypeStruct((rows, half), BF16),
            jax.ShapeDtypeStruct(fresh.shape, F32),
        ),
        in_specs=[vmem] * 4,
        out_specs=(in_hbm, in_hbm),
        scratch_shapes=[pltpu.VMEM((rows, half), BF16), dma, dma],
        compiler_params=pltpu.CompilerParams(vmem_limit_bytes=8 * 1024 * 1024),
        name="store",
    )(blended, stats, scale, fresh)


def solution(mesh):
    in_specs = (
        P("ep", None),
        P("ep", "tp", None, None),
        P(None, "tp"),
        P(None, "tp"),
        P(None, "tp"),
        P(None, "tp"),
        P(None, "tp"),
        P(),
        P("tp", None),
        P(),
        P(),
        P(),
        P(),
        P("ep", None),
        P(("ep", "tp"), None, None),
        P(("ep", "tp"), None, None),
        P(("ep", "tp"), None, None),
    )
    out_specs = (P("ep", "tp"), P("ep", "tp", None, None))
    return jax.shard_map(
        functools.partial(on_device, mesh.shape["ep"], mesh.shape["tp"]),
        mesh=mesh,
        in_specs=in_specs,
        out_specs=out_specs,
        check_vma=False,
    )
```
